32 devices in a mesh: sp: 8 (over z, x), tp: 4 (over y, core).
Axes of the slice: x: 2, y: 2, z: 4, core: 2. Of those that a mesh axis runs over, the one named last changes fastest.
Arguments:
- tokens: bfloat16 [8192, 4096], P('sp'), may hold values from -6 to 6
- input_norm_scale: bfloat16 [4096], replicated, may hold values from 0.099609375 to 1.8984375
- mean_input_weight: bfloat16 [4096, 2048], P('sp', 'tp'), may hold values from -0.09375 to 0.09375
- query_matrix: bfloat16 [4096, 2048], P('sp', 'tp'), may hold values from -0.09375 to 0.09375
- key_matrix: bfloat16 [4096, 2048], P('sp', 'tp'), may hold values from -0.09375 to 0.09375
- value_matrix: bfloat16 [4096, 2048], P('sp', 'tp'), may hold values from -0.09375 to 0.09375
- strength_weight: bfloat16 [4096, 16], P('sp', 'tp'), may hold values from -0.09375 to 0.09375
- decay_input_weight: bfloat16 [4096, 16], P('sp', 'tp'), may hold values from -0.25 to 0.25
- causal_filter_weight: bfloat16 [4, 3, 2048], replicated, may hold values from -3 to 3
- head_decay_logrates: float32 [16], replicated, may hold values from -13.2 to -2.9
- decay_input_shift: float32 [16], replicated, may hold values from -1 to 1
- strength_shift: float32 [16], replicated, may hold values from -5 to -3
- decay_spike: float32 [8192, 16], P('sp', 'tp'), may hold values from -1.3 to 0
- head_norm_scale: bfloat16 [128], replicated, may hold values from 0.099609375 to 1.8984375
- group_mixing_weight: bfloat16 [16, 128, 128], replicated, may hold values from -0.5 to 0.5
- mean_channel_scale: bfloat16 [2048], replicated, may hold values from 0.099609375 to 1.8984375
- mean_output_weight: bfloat16 [2048, 4096], P('tp', 'sp'), may hold values from -0.09375 to 0.09375
- delta_output_weight: bfloat16 [2048, 4096], P('tp', 'sp'), may hold values from -0.09375 to 0.09375
Outputs:
- mixed_out: bfloat16 [8192, 4096], P(('sp', 'tp'))
The draws below stay inside these ranges and needn't reach their ends.
All inputs are finite; a program needn't handle non-finite values.
Results may differ from the reference program's by a relative error of at most 0.015.
Values may be sent and summed in bfloat16 or wider, within the bound.
A program may use at most 128 MiB of HBM per device.

```python
import jax
import jax.numpy as jnp
from jax import lax

D = 4096
POOL_GROUPS = 16
GROUP_DIM = 128
MIXER_HEADS = 16
HEAD_DIM = 128
CONV = 4
BLOCK = 64
TOK_DEV = 1024
POOL_W = 2048
GDN_W = 2048
SEQUENCE_TOKENS = 8192
N_TP = 4


def draw_head_decay_logrates(key, part):
    ranking = jax.random.permutation(jax.random.fold_in(key, 11), MIXER_HEADS)
    fast_count = MIXER_HEADS // 2
    fast_rate = jax.random.uniform(jax.random.fold_in(key, 12), (MIXER_HEADS,), jnp.float32, jnp.log(0.012), jnp.log(0.035))
    slow_rate = jax.random.uniform(jax.random.fold_in(key, 13), (MIXER_HEADS,), jnp.float32, jnp.log(2e-06), jnp.log(2e-05))
    return jnp.where(ranking < fast_count, fast_rate, slow_rate).astype(jnp.float32)


def draw_decay_spike(key, part):
    block_ids = jnp.arange(SEQUENCE_TOKENS) // TOK_DEV
    block_rates = jnp.exp(jax.random.uniform(jax.random.fold_in(key, 21), (SEQUENCE_TOKENS // TOK_DEV, MIXER_HEADS), jnp.float32, jnp.log(1e-06), jnp.log(2e-05)))
    stable_portion = -block_rates[block_ids]
    spike_rows = jax.random.randint(jax.random.fold_in(key, 22), (2, MIXER_HEADS), 0, SEQUENCE_TOKENS)
    error_values = jax.random.uniform(jax.random.fold_in(key, 23), (2, MIXER_HEADS), jnp.float32, 0.2, 0.45)
    match_flags = jnp.arange(SEQUENCE_TOKENS)[:, None, None] == spike_rows[None, :, :]
    spike_portion = jnp.sum(jnp.where(match_flags, jnp.log(1.0 - error_values)[None, :, :], 0.0), axis=1)
    return (stable_portion + spike_portion).astype(jnp.float32)


def block_levels(stream_key, dims, split, smallest, largest):
    factor_of, own = 1.0, jax.random.fold_in(stream_key, 6)
    for dim, shards_of in split:
        heights = jnp.exp(jax.random.uniform(jax.random.fold_in(own, dim), (shards_of,), jnp.float32, smallest / len(split), largest / len(split)))
        factor_of = factor_of * jnp.repeat(heights, dims[dim] // shards_of).reshape([-1 if axis == dim else 1 for axis in range(len(dims))])
    return factor_of


def bell_draw(own_key, shape, scale, reach, split=(), held_as=jnp.bfloat16):
    drawn = jax.random.normal(own_key, shape, jnp.float32) * scale
    if len(split) > 0:
        drawn = block_levels(own_key, shape, split, -0.22, 0.18) * drawn
    return jnp.clip(drawn, min=-reach, max=reach).astype(held_as)


def setup_inputs(seed: int = 0) -> dict:
    seeds = jax.random.split(jax.random.key(seed), 19)
    return {
        "tokens": bell_draw(seeds[0], (SEQUENCE_TOKENS, D), 1.0, 6.0, ((0, 8),)),
        "input_norm_scale": jnp.clip(1.0 + 0.18 * jax.random.normal(seeds[1], (D,), jnp.float32), 0.099609375, 1.8984375).astype(jnp.bfloat16),
        "mean_input_weight": bell_draw(seeds[2], (D, POOL_W), D ** -0.5, 0.09375, ((0, 8), (1, 4))),
        "query_matrix": bell_draw(seeds[3], (D, GDN_W), D ** -0.5, 0.09375, ((0, 8), (1, 4))),
        "key_matrix": bell_draw(seeds[4], (D, GDN_W), D ** -0.5, 0.09375, ((0, 8), (1, 4))),
        "value_matrix": bell_draw(seeds[5], (D, GDN_W), D ** -0.5, 0.09375, ((0, 8), (1, 4))),
        "strength_weight": bell_draw(seeds[6], (D, MIXER_HEADS), D ** -0.5, 0.09375, ((0, 8), (1, 4))),
        "decay_input_weight": bell_draw(seeds[7], (D, MIXER_HEADS), (D // 9) ** -0.5, 0.25, ((0, 8), (1, 4))),
        "causal_filter_weight": bell_draw(seeds[8], (CONV, 3, GDN_W), CONV ** -0.5, 3.0),
        "head_decay_logrates": draw_head_decay_logrates(jax.random.fold_in(seeds[18], 71), 0),
        "decay_input_shift": jnp.clip(jax.random.uniform(seeds[10], (MIXER_HEADS,), jnp.float32, -1.0, 1.0), -1.0, 1.0),
        "strength_shift": jnp.clip(jax.random.uniform(seeds[11], (MIXER_HEADS,), jnp.float32, -5.0, -3.0), -5.0, -3.0),
        "decay_spike": draw_decay_spike(jax.random.fold_in(seeds[18], 71), 0),
        "head_norm_scale": jnp.clip(1.0 + 0.18 * jax.random.normal(seeds[13], (HEAD_DIM,), jnp.float32), 0.099609375, 1.8984375).astype(jnp.bfloat16),
        "group_mixing_weight": bell_draw(seeds[14], (POOL_GROUPS, GROUP_DIM, GROUP_DIM), GROUP_DIM ** -0.5, 0.5),
        "mean_channel_scale": jnp.clip(1.0 + 0.18 * jax.random.normal(seeds[15], (POOL_W,), jnp.float32), 0.099609375, 1.8984375).astype(jnp.bfloat16),
        "mean_output_weight": bell_draw(seeds[16], (POOL_W, D), (POOL_W + GDN_W) ** -0.5, 0.09375, ((0, 4), (1, 8))),
        "delta_output_weight": bell_draw(seeds[17], (GDN_W, D), (POOL_W + GDN_W) ** -0.5, 0.09375, ((0, 4), (1, 8))),
    }


EPSILON = 1e-06

def scale_rows(values, gain_vec):
    squares = lax.optimization_barrier(jnp.mean(values * values, axis=-1, keepdims=True))
    return values * lax.rsqrt(squares + EPSILON) * gain_vec.astype(jnp.float32)

def unit_rows(values):
    return values * lax.rsqrt(lax.optimization_barrier(jnp.sum(values * values, axis=-1, keepdims=True)) + EPSILON)

def causal_taps(extended, taps, rows_out):
    tap_sum = jnp.zeros((rows_out, taps.shape[1]), jnp.float32)
    for tap_index in range(taps.shape[0]):
        tap_sum = tap_sum + taps[tap_index] * extended[tap_index:tap_index + rows_out]
    return jax.nn.silu(tap_sum)

def pool_means(previous, current, group_ids, positions):
    pool_reach = 15
    rows_out = current.shape[0]
    extended = jnp.concatenate([previous, current], axis=0).astype(jnp.float32)
    window_size = jnp.left_shift(jnp.int32(2), (group_ids % 4).astype(jnp.int32))
    windowed = jnp.zeros(current.shape, jnp.float32)
    for lag_rows in range(pool_reach + 1):
        shifted = extended[pool_reach - lag_rows:pool_reach - lag_rows + rows_out]
        windowed = windowed + jnp.where(lag_rows < window_size[None, :], shifted, 0.0)
    counts = jnp.minimum(positions[:, None] + 1, window_size[None, :]).astype(jnp.float32)
    return (windowed / counts - extended[pool_reach:]).astype(jnp.bfloat16)

def block_terms(query, keys, values, decay_logarithm, beta):
    blocks = keys.shape[0] // BLOCK

    def to_blocks(tensor):
        return jnp.swapaxes(tensor.reshape((blocks, BLOCK) + tensor.shape[1:]), 1, 2)
    query_b = to_blocks(query)
    keys_b = to_blocks(keys)
    values_b = to_blocks(values)
    decay_b = to_blocks(decay_logarithm)
    beta_b = to_blocks(beta)
    cumulative = jnp.cumsum(decay_b, axis=-1)
    positions = jnp.arange(BLOCK)
    causal = positions[:, None] >= positions[None, :]
    strict = positions[:, None] > positions[None, :]
    spread = cumulative[..., :, None] - cumulative[..., None, :]
    weights = jnp.where(causal, jnp.exp(jnp.where(causal, spread, 0.0)), 0.0)
    keys_beta = keys_b * beta_b[..., None]
    values_beta = values_b * beta_b[..., None]
    intersection = jnp.einsum('nhid,nhjd->nhij', keys_beta, keys_b, precision=lax.Precision.HIGHEST)
    lower_part = jnp.where(strict, intersection * weights, 0.0) + jnp.eye(BLOCK, dtype=jnp.float32)
    right_side = jnp.concatenate([values_beta, keys_beta * jnp.exp(cumulative)[..., None]], axis=-1)
    solved = jax.scipy.linalg.solve_triangular(lower_part, right_side, lower=True, unit_diagonal=True)
    value_depth = values.shape[-1]
    update = solved[..., :value_depth]
    project = solved[..., value_depth:]
    scores = jnp.einsum('nhid,nhjd->nhij', query_b, keys_b, precision=lax.Precision.HIGHEST) * weights
    query_dec = query_b * jnp.exp(cumulative)[..., None]
    keys_dec = keys_b * jnp.exp(cumulative[..., -1:] - cumulative)[..., None]
    carry_decay = jnp.exp(cumulative[..., -1])
    return (scores, query_dec, keys_dec, update, project, carry_decay)

def run_blocks(state, terms):

    def advance(carried, inputs):
        scores, query_dec, keys_dec, update, project, carry_decay = inputs
        fresh = update - jnp.einsum('hcd,hde->hce', project, carried, precision=lax.Precision.HIGHEST)
        output = jnp.einsum('hcd,hde->hce', query_dec, carried, precision=lax.Precision.HIGHEST)
        output = output + jnp.einsum('hij,hje->hie', scores, fresh, precision=lax.Precision.HIGHEST)
        carried = carried * carry_decay[:, None, None] + jnp.einsum('hcd,hce->hde', keys_dec, fresh, precision=lax.Precision.HIGHEST)
        return (carried, output)
    final_state, outputs = lax.scan(advance, state, terms)
    return outputs

def reference(tokens, input_norm_scale, mean_input_weight, query_matrix, key_matrix, value_matrix, strength_weight, decay_input_weight, causal_filter_weight, head_decay_logrates, decay_input_shift, strength_shift, decay_spike, head_norm_scale, group_mixing_weight, mean_channel_scale, mean_output_weight, delta_output_weight):
    normed = scale_rows(tokens.astype(jnp.float32), input_norm_scale).astype(jnp.bfloat16)
    pool_raw = jnp.dot(normed.astype(jnp.float32), mean_input_weight.astype(jnp.float32), preferred_element_type=jnp.float32).astype(jnp.bfloat16)
    query_raw = jnp.dot(normed.astype(jnp.float32), query_matrix.astype(jnp.float32), preferred_element_type=jnp.float32).astype(jnp.bfloat16)
    key_raw = jnp.dot(normed.astype(jnp.float32), key_matrix.astype(jnp.float32), preferred_element_type=jnp.float32).astype(jnp.bfloat16)
    value_raw = jnp.dot(normed.astype(jnp.float32), value_matrix.astype(jnp.float32), preferred_element_type=jnp.float32).astype(jnp.bfloat16)
    beta_raw = jnp.dot(normed.astype(jnp.float32), strength_weight.astype(jnp.float32), preferred_element_type=jnp.float32).astype(jnp.bfloat16)
    decay_unshaped = jnp.dot(normed.astype(jnp.float32), decay_input_weight.astype(jnp.float32), preferred_element_type=jnp.float32).astype(jnp.bfloat16)
    qkv_raw = jnp.concatenate([query_raw, key_raw, value_raw], axis=1)
    extended_qkv = jnp.concatenate([jnp.zeros((CONV - 1, 3 * GDN_W), jnp.bfloat16), qkv_raw], axis=0).astype(jnp.float32)
    convolved = causal_taps(extended_qkv, causal_filter_weight.reshape(CONV, 3 * GDN_W).astype(jnp.float32), SEQUENCE_TOKENS)
    query = unit_rows(convolved[:, :GDN_W].reshape(SEQUENCE_TOKENS, MIXER_HEADS, HEAD_DIM)) * HEAD_DIM ** (-0.5)
    keys = unit_rows(convolved[:, GDN_W:2 * GDN_W].reshape(SEQUENCE_TOKENS, MIXER_HEADS, HEAD_DIM))
    values = convolved[:, 2 * GDN_W:].reshape(SEQUENCE_TOKENS, MIXER_HEADS, HEAD_DIM)
    beta = jax.nn.sigmoid(beta_raw.astype(jnp.float32) + strength_shift)
    decay_logarithm = -jnp.exp(head_decay_logrates) * jax.nn.softplus(decay_unshaped.astype(jnp.float32) + decay_input_shift) + decay_spike
    terms = block_terms(query, keys, values, decay_logarithm, beta)
    outputs = run_blocks(jnp.zeros((MIXER_HEADS, HEAD_DIM, HEAD_DIM), jnp.float32), terms)
    delta_rows = jnp.swapaxes(outputs, 1, 2).reshape(SEQUENCE_TOKENS, MIXER_HEADS, HEAD_DIM)
    delta_mixed = scale_rows(delta_rows, head_norm_scale).astype(jnp.bfloat16).reshape(SEQUENCE_TOKENS, GDN_W)
    group_ids = (jnp.arange(POOL_W) // GROUP_DIM).astype(jnp.int32)
    positions = jnp.arange(SEQUENCE_TOKENS).astype(jnp.int32)
    pool_diff = pool_means(jnp.zeros((15, POOL_W), jnp.bfloat16), pool_raw, group_ids, positions)
    pooled = jnp.einsum('tgc,gcd->tgd', pool_diff.astype(jnp.float32).reshape(SEQUENCE_TOKENS, POOL_GROUPS, GROUP_DIM), group_mixing_weight.astype(jnp.float32))
    pool_mixed = (pooled.reshape(SEQUENCE_TOKENS, POOL_W) * mean_channel_scale.astype(jnp.float32)).astype(jnp.bfloat16)
    pool_slice = POOL_W // N_TP
    delta_slice = GDN_W // N_TP
    summed = jnp.zeros((SEQUENCE_TOKENS, D), jnp.float32)
    for shard_index in range(N_TP):
        pool_part = pool_mixed[:, shard_index * pool_slice:(shard_index + 1) * pool_slice]
        delta_part = delta_mixed[:, shard_index * delta_slice:(shard_index + 1) * delta_slice]
        rows_in = jnp.concatenate([pool_part, delta_part], axis=1)
        weight_rows = jnp.concatenate([mean_output_weight[shard_index * pool_slice:(shard_index + 1) * pool_slice], delta_output_weight[shard_index * delta_slice:(shard_index + 1) * delta_slice]], axis=0)
        partial_sum = jnp.dot(rows_in.astype(jnp.float32), weight_rows.astype(jnp.float32), preferred_element_type=jnp.float32).astype(jnp.bfloat16)
        summed = summed + partial_sum.astype(jnp.float32)
    return summed.astype(jnp.bfloat16)
```

```python
import jax
import jax.numpy as jnp
from jax import lax
from jax.experimental import pallas as pl
from jax.experimental.pallas import tpu as pltpu
from jax.sharding import PartitionSpec as P

GROUP_DIM = 128
CONV = 4
EPSILON = 1e-06
PAD = 16
CHUNK = 128
BF16 = jnp.bfloat16
F32 = jnp.float32
MESH = pl.DeviceIdType.MESH
KEY, VAL, QRY, POOL = range(4)


def dot(left, right):
    return jnp.dot(left.astype(BF16), right.astype(BF16), preferred_element_type=F32)


def dot_nt(left, right):
    return lax.dot_general(
        left.astype(BF16),
        right.astype(BF16),
        (((1,), (1,)), ((), ())),
        preferred_element_type=F32,
    )


def dot_tn(left, right):
    return lax.dot_general(
        left.astype(BF16),
        right.astype(BF16),
        (((0,), (0,)), ((), ())),
        preferred_element_type=F32,
    )


def unit_rows(values):
    return values * lax.rsqrt(jnp.sum(values * values, axis=-1, keepdims=True) + EPSILON)


def delta_chunk(heads, depth, chunk, qkv, taps, beta, decay, carry):
    width = heads * depth
    row = lax.broadcasted_iota(jnp.int32, (chunk, chunk), 0)
    col = lax.broadcasted_iota(jnp.int32, (chunk, chunk), 1)
    causal = row >= col
    strict = row > col
    eye = jnp.where(row == col, 1.0, 0.0)
    convolved = []
    for r in range(3):
        extended = qkv[r].astype(F32)
        total = jnp.zeros((chunk, width), F32)
        for i in range(CONV):
            start = PAD - (CONV - 1) + i
            total = total + taps[i][r] * extended[start : start + chunk]
        convolved.append(total / (1.0 + jnp.exp(-total)))
    tri = jnp.where(causal, 1.0, 0.0)
    cum_cols = jnp.dot(tri, decay, preferred_element_type=F32, precision=lax.Precision.HIGHEST)
    cum_rows = lax.dot_general(
        decay,
        tri,
        (((0,), (1,)), ((), ())),
        preferred_element_type=F32,
        precision=lax.Precision.HIGHEST,
    )
    base = min(16, chunk)
    hs = range(heads)
    q = [unit_rows(convolved[0][:, h * depth : (h + 1) * depth]) * depth ** (-0.5) for h in hs]
    k = [unit_rows(convolved[1][:, h * depth : (h + 1) * depth]) for h in hs]
    v = [convolved[2][:, h * depth : (h + 1) * depth] for h in hs]
    cum = [cum_cols[:, h : h + 1] for h in hs]
    last = [cum_cols[chunk - 1 : chunk, h : h + 1] for h in hs]
    beta = [beta[:, h : h + 1] for h in hs]
    weights = [
        jnp.where(causal, jnp.exp(jnp.where(causal, cum[h] - cum_rows[h : h + 1, :], 0.0)), 0.0)
        for h in hs
    ]
    kb = [k[h] * beta[h] for h in hs]
    lower = [jnp.where(strict, dot_nt(kb[h], k[h]) * weights[h], 0.0) for h in hs]
    power = [jnp.where(row // base == col // base, lower[h], 0.0) for h in hs]
    inverse = [eye - power[h] for h in hs]
    reach = 2
    while reach < base:
        power = [dot(power[h], power[h]) for h in hs]
        inverse = [inverse[h] + dot(inverse[h], power[h]) for h in hs]
        reach *= 2
    size = base
    while size < chunk:
        pair = (row // (2 * size) == col // (2 * size)) & (row // size != col // size)
        right = [dot(jnp.where(pair, lower[h], 0.0), inverse[h]) for h in hs]
        inverse = [inverse[h] - dot(inverse[h], right[h]) for h in hs]
        size *= 2
    grow = [jnp.exp(cum[h]) for h in hs]
    sides = [jnp.concatenate([v[h] * beta[h], kb[h] * grow[h]], axis=1) for h in hs]
    solved = [dot(inverse[h], sides[h]) for h in hs]
    scores = [dot_nt(q[h], k[h]) * weights[h] for h in hs]
    kd = [k[h] * jnp.exp(last[h] - cum[h]) for h in hs]
    zeros = jnp.zeros((chunk, depth), F32)
    state = [carry[h] for h in hs]
    fresh = [
        jnp.concatenate([solved[h][:, :depth], zeros], axis=1) - dot(solved[h][:, depth:], state[h])
        for h in hs
    ]
    outs = [dot(q[h] * grow[h], state[h]) + dot(scores[h], fresh[h]) for h in hs]
    for h in hs:
        carry[h] = state[h] * jnp.exp(last[h]) + dot_tn(kd[h], fresh[h])
    return outs


class Ring:
    def __init__(self, hops, half_rows, refs, sems, owner, peers, window):
        self.refs, self.sems, self.owner, self.peers, self.window = refs, sems, owner, peers, window
        self.items = []
        self.index = {}
        rows_in, rows_out = half_rows
        for j in range(1, hops + 1):
            for m in (KEY, VAL, QRY):
                top = rows_in // 2
                full = rows_in + PAD if m == KEY else rows_in
                if j < hops:
                    self.add(("in", m, 0), j, [("in", m, 0, full)] * 2)
                else:
                    self.add(("in", m, 0), j, [("in", m, 0, top), ("in", m, top, full)])
        top = rows_in // 2
        for j in range(1, hops + 1):
            if j < hops:
                self.add(("in", POOL, 0), j, [("in", POOL, 0, top)] * 2)
                self.add(("in", POOL, 1), j, [("in", POOL, top, rows_in)] * 2)
            else:
                self.add(("in", POOL, 0), j, [("in", POOL, 0, top), ("in", POOL, top, rows_in)])
        for j in range(1, hops + 1):
            if j < hops:
                self.add(("out", 0, 0), j, [("out", 0, 0, rows_out)] * 2)
                self.add(("out", 1, 0), j, [("out", 1, 0, rows_out)] * 2)
            else:
                self.add(("out", 0, 0), j, [("out", 0, 0, rows_out), ("out", 1, 0, rows_out)])
        self.finish = []
        total = 0
        for _, _, parts in self.items:
            total += parts[0][3] - parts[0][2]
            self.finish.append(total)
        self.total = total
        self.started = 0
        self.sent = set()
        self.received = set()

    def add(self, key, j, parts):
        self.index[key + (j,)] = len(self.items)
        self.items.append((key, j, parts))

    def copy(self, i, side):
        key, j, parts = self.items[i]
        kind, m, low, high = parts[side]
        ref = self.refs[kind]
        block = ref.at[m, self.owner(-(j - 1) if side == 0 else j - 1), pl.ds(low, high - low), :]
        return pltpu.make_async_remote_copy(
            src_ref=block,
            dst_ref=block,
            send_sem=self.sems[0].at[i, side],
            recv_sem=self.sems[1].at[i, side],
            device_id=self.peers[side],
            device_id_type=MESH,
        )

    def arrive(self, i, side):
        if (i, side) in self.received:
            return
        self.received.add((i, side))
        self.copy(i, side).wait_recv()

    def leave(self, i):
        if i in self.sent:
            return
        self.sent.add(i)
        for side in range(2):
            self.copy(i, side).wait_send()

    def start_next(self):
        i = self.started
        if i >= len(self.items):
            return
        if i >= self.window:
            self.leave(i - self.window)
        key, j, parts = self.items[i]
        for side in range(2):
            if j > 1:
                kind, m, low, high = parts[side]
                for before in range(i):
                    other, hop, pieces = self.items[before]
                    if hop == j - 1 and pieces[side][:2] == (kind, m) and pieces[side][2] <= low < pieces[side][3]:
                        self.arrive(before, side)
                    elif hop == j - 1 and pieces[side][:2] == (kind, m) and low <= pieces[side][2] < high:
                        self.arrive(before, side)
            self.copy(i, side).start()
        self.started += 1

    def tick(self, part):
        while self.started < len(self.items):
            behind = self.started - self.window
            if behind >= 0 and self.finish[behind] > part * self.total:
                break
            self.start_next()

    def need(self, key):
        i = self.index[key]
        while self.started < min(len(self.items), i + self.window + 1):
            self.start_next()
        for side in range(2):
            self.arrive(i, side)

    def close(self):
        while self.started < len(self.items):
            self.start_next()
        for i in range(len(self.items)):
            for side in range(2):
                self.arrive(i, side)
            self.leave(i)


def mixer_kernel(cfg, *refs):
    (
        tok_ref, gain_ref, wk_ref, wv_ref, wq_ref, wp_ref, narrow_ref, tap_ref, rate_ref, dshift_ref,
        sshift_ref, spike_ref, hgain_ref, gmw_ref, cscale_ref, wpo_ref, wdo_ref,
    ) = refs[:17]
    out_ref = refs[17]
    (
        win, wout, normed, acc, raw, stage, nraw, gmw, carry, held, caught, psend, corerecv, ysend, yrecv,
        obuf, ring_send, ring_recv, local_sem, tok_sem, halo_send, halo_recv, scan_send, scan_recv,
        core_send, core_recv, y_send, y_recv, out_sem,
    ) = refs[18:]
    n_sp, n_tp, heads, depth, grid_x = cfg
    grid_z = n_sp // grid_x
    hops = n_sp // 2
    n_y = n_tp // 2
    rows, width = raw.shape[1] - PAD, raw.shape[2]
    rows_in = normed.shape[2]
    cols_out = wout.shape[3]
    share = rows // n_tp
    sp = lax.axis_index("sp")
    tp = lax.axis_index("tp")
    core = tp % 2
    ypos = tp // 2

    def sp_at(r):
        s = jnp.maximum(r - grid_z, 0)
        i = s // (grid_x - 1)
        k = s % (grid_x - 1)
        x = 1 + jnp.where(i % 2 == 0, k, grid_x - 2 - k)
        return jnp.where(r < grid_z, r * grid_x, (grid_z - 1 - i) * grid_x + x)

    zc = sp // grid_x
    xc = sp % grid_x
    ic = grid_z - 1 - zc
    kc = jnp.where(ic % 2 == 0, xc - 1, grid_x - 1 - xc)
    pos = jnp.where(xc == 0, zc, grid_z + ic * (grid_x - 1) + kc)

    def owner(offset):
        return sp_at((pos + offset + n_sp) % n_sp)

    locals_ = []

    def bring(src, dst):
        locals_.append(pltpu.make_async_copy(src, dst, local_sem.at[len(locals_)]))
        locals_[-1].start()

    bring(wk_ref, win.at[KEY, sp, pl.ds(0, rows_in), :])
    bring(narrow_ref, win.at[KEY, sp, pl.ds(rows_in, PAD), :])
    bring(wv_ref, win.at[VAL, sp, pl.ds(0, rows_in), :])
    bring(wq_ref, win.at[QRY, sp, pl.ds(0, rows_in), :])
    bring(wp_ref, win.at[POOL, sp, pl.ds(0, rows_in), :])
    bring(wpo_ref, wout.at[0, sp])
    bring(wdo_ref, wout.at[1, sp])
    groups = gmw.shape[0]
    bring(gmw_ref.at[pl.ds(tp * groups, groups)], gmw)
    step_rows = stage.shape[1]
    n_stage = rows // step_rows

    def token_copy(t, slot):
        return pltpu.make_async_copy(
            tok_ref.at[pl.ds(pl.multiple_of(t * step_rows, step_rows), step_rows), :],
            stage.at[slot],
            tok_sem.at[slot],
        )

    token_copy(0, 0).start()

    barrier = pltpu.get_barrier_semaphore()
    for k in range(1, n_sp):
        pl.semaphore_signal(barrier, inc=1, device_id=((sp + k) % n_sp, tp), device_id_type=MESH)
    for k in range(1, n_tp):
        pl.semaphore_signal(barrier, inc=1, device_id=(sp, (tp + k) % n_tp), device_id_type=MESH)
    for c in locals_:
        c.wait()
    pl.semaphore_wait(barrier, n_sp + n_tp - 2)

    ring = Ring(
        hops,
        (rows_in, wout.shape[2]),
        {"in": win, "out": wout},
        (ring_send, ring_recv),
        owner,
        [(owner(1), tp), (owner(-1), tp)],
        2,
    )
    ring.tick(0.0)

    def norm_step(t, _):
        slot = t % 2
        token_copy(t, slot).wait()

        @pl.when(t + 1 < n_stage)
        def _():
            token_copy(t + 1, 1 - slot).start()

        def piece(u, _):
            at = pl.ds(pl.multiple_of(u * 32, 32), 32)
            squares = jnp.zeros((32, 1), F32)
            for b in range(n_sp):
                x = stage[slot, at, b * rows_in : (b + 1) * rows_in].astype(F32)
                squares = squares + jnp.sum(x * x, axis=-1, keepdims=True)
            scale = lax.rsqrt(squares * (1.0 / (n_sp * rows_in)) + EPSILON)
            to = pl.ds(pl.multiple_of(t * step_rows + u * 32, 32), 32)
            for b in range(n_sp):
                cols = slice(b * rows_in, (b + 1) * rows_in)
                x = stage[slot, at, cols].astype(F32)
                normed[b, to, :] = (x * scale * gain_ref[:, cols].astype(F32)).astype(BF16)
            return 0

        lax.fori_loop(0, step_rows // 32, piece, 0)
        return 0

    lax.fori_loop(0, n_stage, norm_step, 0)

    tile = min(256, rows)
    n_tile = rows // tile

    def project(m, owners, first=False, final=False):
        def body(t, _):
            at = pl.ds(pl.multiple_of(t * tile, tile), tile)
            total = None if first else acc[m, at, :]
            for o in owners:
                term = jnp.dot(
                    normed[o, at, :], win[m, o, pl.ds(0, rows_in), :], preferred_element_type=F32
                )
                total = term if total is None else total + term
            if final:
                raw[m, pl.ds(pl.multiple_of(PAD + t * tile, PAD), tile), :] = total.astype(BF16)
            else:
                acc[m, at, :] = total
            return 0

        lax.fori_loop(0, n_tile, body, 0)

    def halo(m):
        return pltpu.make_async_remote_copy(
            src_ref=raw.at[m, pl.ds(rows, PAD), :],
            dst_ref=raw.at[m, pl.ds(0, PAD), :],
            send_sem=halo_send.at[m],
            recv_sem=halo_recv.at[m],
            device_id=((sp + 1) % n_sp, tp),
            device_id_type=MESH,
        )

    def halo_start(m):
        @pl.when(sp + 1 < n_sp)
        def _():
            halo(m).start()

        @pl.when(sp == 0)
        def _():
            raw[m, pl.ds(0, PAD), :] = jnp.zeros((PAD, width), BF16)

    def halo_wait(m):
        @pl.when(sp > 0)
        def _():
            halo(m).wait_recv()

    def own(m, _):
        project(m, [sp], first=True)
        return 0

    lax.fori_loop(0, 4, own, 0)

    def arriving(i, _):
        for k in range(3 * hops):
            @pl.when(i == k)
            def _():
                ring.need(("in", k % 3, 0, k // 3 + 1))

        m, j = i % 3, i // 3 + 1

        @pl.when(j < hops)
        def _():
            project(m, [owner(-j), owner(j)])

        @pl.when(j == hops)
        def _():
            project(m, [owner(hops)], final=True)
            for k in range(3):
                @pl.when(m == k)
                def _():
                    halo_start(k)

        return 0

    lax.fori_loop(0, 3 * hops, arriving, 0)

    def narrow_body(t, _):
        at = pl.ds(pl.multiple_of(t * tile, tile), tile)
        total = jnp.zeros((tile, PAD), F32)
        for o in range(n_sp):
            total = total + dot_nt(normed[o, at, :], win[KEY, o, pl.ds(rows_in, PAD), :])
        nraw[at, :] = total
        return 0

    lax.fori_loop(0, n_tile, narrow_body, 0)

    lane = lax.broadcasted_iota(jnp.int32, (1, rate_ref.shape[1]), 1)
    small = lax.broadcasted_iota(jnp.int32, (1, heads), 1)

    def head_row(ref):
        total = jnp.zeros((1, heads), F32)
        for h in range(heads):
            value = jnp.sum(jnp.where(lane == tp * heads + h, ref[...], 0.0), axis=-1, keepdims=True)
            total = total + jnp.where(small == h, value, 0.0)
        return total

    speed = -jnp.exp(head_row(rate_ref))
    dshift = head_row(dshift_ref)
    sshift = head_row(sshift_ref)
    mine = pl.ds(pl.multiple_of(tp * width, 128), width)
    wide = lax.broadcasted_iota(jnp.int32, (depth, 2 * depth), 1)
    sub = lax.broadcasted_iota(jnp.int32, (depth, 2 * depth), 0)
    for h in range(heads):
        carry[h] = jnp.where(wide == sub + depth, 1.0, 0.0)
    for m in (KEY, VAL, QRY):
        halo_wait(m)
    chunk = min(CHUNK, rows)
    n_chunk = rows // chunk
    done_in = 3.0 / 6.0

    def delta_step(c, _):
        for k in range(n_chunk):
            @pl.when(c == k)
            def _():
                ring.tick(done_in + 0.03 + 0.11 * k / n_chunk)

        at = pl.ds(pl.multiple_of(c * chunk, chunk), chunk)
        window = pl.ds(pl.multiple_of(c * chunk, chunk), chunk + PAD)
        qkv = [raw[m, window, :] for m in (QRY, KEY, VAL)]
        taps = [[tap_ref[i, r : r + 1, mine].astype(F32) for r in range(3)] for i in range(CONV)]
        narrow = nraw[at, :].astype(BF16).astype(F32)
        beta = 1.0 / (1.0 + jnp.exp(-(narrow[:, :heads] + sshift)))
        x = narrow[:, heads : 2 * heads] + dshift
        soft = jnp.maximum(x, 0.0) + jnp.log1p(jnp.exp(-jnp.abs(x)))
        decay = speed * soft + spike_ref[at, :]
        outs = delta_chunk(heads, depth, chunk, qkv, taps, beta, decay, carry)
        for h in range(heads):
            cols = slice(h * depth, (h + 1) * depth)
            acc[0, at, cols] = outs[h][:, :depth]
            acc[1, at, cols] = outs[h][:, depth:]
        return 0

    lax.fori_loop(0, n_chunk, delta_step, 0)

    def halo_leave(m):
        @pl.when(sp + 1 < n_sp)
        def _():
            halo(m).wait_send()

    for m in (KEY, VAL, QRY):
        halo_leave(m)

    distances = [1]
    while 2 * distances[-1] < n_sp - 1:
        distances.append(2 * distances[-1])
    shifts = [1] + distances
    n_round = len(shifts)

    def scan_copy(r, source):
        last = r == n_round - 1
        pick = pl.ds(0, depth if last else 2 * depth)
        return pltpu.make_async_remote_copy(
            src_ref=source.at[:, :, pick],
            dst_ref=caught.at[r, :, :, pick],
            send_sem=scan_send.at[r],
            recv_sem=scan_recv.at[r],
            device_id=((sp + shifts[r]) % n_sp, tp),
            device_id_type=MESH,
        )

    def scan_start(r, source):
        @pl.when(sp + shifts[r] < n_sp)
        def _():
            scan_copy(r, source).start()

    def scan_wait(r, source):
        @pl.when(sp >= shifts[r])
        def _():
            scan_copy(r, source).wait_recv()

        @pl.when(sp < shifts[r])
        def _():
            caught[r] = jnp.zeros(caught.shape[1:], BF16)

    pool_hops = []
    for j in range(1, hops):
        pool_hops.append(j)
    for h in range(heads):
        held[0, h] = carry[h].astype(BF16)
    sources = [held.at[0]]
    scan_start(0, sources[0])

    def pool_hop(j):
        if j < hops:
            ring.need(("in", POOL, 0, j))
            ring.need(("in", POOL, 1, j))
            project(POOL, [owner(-j), owner(j)])
        else:
            ring.need(("in", POOL, 0, j))
            project(POOL, [owner(hops)], final=True)
            halo_start(POOL)

    per_round = max(1, -(-hops // max(1, n_round - 1)))
    next_hop = 1
    for r in range(n_round):
        while next_hop <= hops and next_hop <= per_round * (r + 1) and r < n_round - 1:
            pool_hop(next_hop)
            next_hop += 1
        if r == n_round - 1:
            while next_hop <= hops:
                pool_hop(next_hop)
                next_hop += 1
            ring.tick(done_in + 0.22)
            halo_wait(POOL)
            pool_mix(
                cfg, raw, gmw, cscale_ref, sp, tp, tile, rows, width,
            )
        scan_wait(r, sources[r])
        if r == 0:
            sources.append(caught.at[0])
        elif r < n_round - 1:
            before = sources[r]
            for h in range(heads):
                later = before[h]
                own_part = later[:, :depth].astype(F32)
                pushed = dot(later[:, depth:], caught[r, h])
                held[r, h, :, pl.ds(0, depth)] = (own_part + pushed[:, :depth]).astype(BF16)
                held[r, h, :, pl.ds(depth, depth)] = pushed[:, depth:].astype(BF16)
            sources.append(held.at[r])
        else:
            before = sources[r]
            for h in range(heads):
                later = before[h]
                pushed = dot(later[:, depth:], caught[r, h, :, pl.ds(0, depth)])
                held[r, h, :, pl.ds(0, depth)] = (later[:, :depth].astype(F32) + pushed).astype(BF16)
        if r + 1 < n_round:
            scan_start(r + 1, sources[r + 1])
    incoming = held.at[n_round - 1]
    ring.tick(done_in + 0.26)

    hgain = hgain_ref[...].astype(F32)

    def finish_step(t, _):
        at = pl.ds(pl.multiple_of(t * tile, tile), tile)
        to = pl.ds(pl.multiple_of(PAD + t * tile, PAD), tile)
        for h in range(heads):
            cols = slice(h * depth, (h + 1) * depth)
            value = acc[0, at, cols] + dot(acc[1, at, cols], incoming[h, :, pl.ds(0, depth)])
            scale = lax.rsqrt(jnp.mean(value * value, axis=-1, keepdims=True) + EPSILON)
            raw[VAL, to, cols] = (value * scale * hgain).astype(BF16)
        return 0

    lax.fori_loop(0, n_tile, finish_step, 0)

    def block_of(k):
        step = (k + 1) // 2
        return owner(jnp.where(k % 2 == 1, -step, step))

    def partial(dest, o):
        at = pl.ds(pl.multiple_of(PAD + dest * share, PAD), share)
        return jnp.dot(raw[KEY, at, :], wout[0, o], preferred_element_type=F32) + jnp.dot(
            raw[VAL, at, :], wout[1, o], preferred_element_type=F32
        )

    def core_copy(k):
        return pltpu.make_async_remote_copy(
            src_ref=psend.at[k % 2],
            dst_ref=corerecv.at[k],
            send_sem=core_send.at[k],
            recv_sem=core_recv.at[k],
            device_id=(sp, ypos * 2 + 1 - core),
            device_id_type=MESH,
        )

    def y_copy(k, d):
        return pltpu.make_async_remote_copy(
            src_ref=ysend.at[k, d - 1],
            dst_ref=yrecv.at[k, d - 1],
            send_sem=y_send.at[k, d - 1],
            recv_sem=y_recv.at[k, d - 1],
            device_id=(sp, ((ypos + d) % n_y) * 2 + core),
            device_id_type=MESH,
        )

    def out_copy(k):
        return pltpu.make_async_copy(
            obuf.at[k % 2],
            out_ref.at[:, pl.ds(pl.multiple_of(block_of(k) * cols_out, 128), cols_out)],
            out_sem.at[k % 2],
        )

    own_rows = acc

    def own_at(k, y):
        flat = (k % 2) * n_y + y
        return own_rows.at[2, pl.ds(pl.multiple_of(flat * share, share), share), pl.ds(0, cols_out)]

    def stage_one(k):
        o = block_of(k)

        @pl.when(k >= 2)
        def _():
            core_copy(k - 2).wait_send()

        for y in range(n_y):
            psend[k % 2, y] = partial(y * 2 + 1 - core, o).astype(BF16)
        core_copy(k).start()

    def stage_two(k):
        o = block_of(k)
        mine_now = partial(ypos * 2 + core, o).astype(BF16).astype(F32)
        parts = [partial(((ypos + d) % n_y) * 2 + core, o).astype(BF16).astype(F32) for d in range(1, n_y)]
        core_copy(k).wait_recv()
        for d in range(1, n_y):
            there = (ypos + d) % n_y
            ysend[k, d - 1] = (parts[d - 1] + corerecv[k, there].astype(F32)).astype(BF16)
            y_copy(k, d).start()
        own_at(k, 0)[...] = mine_now + corerecv[k, ypos].astype(F32)

    def stage_three(k):
        total = own_at(k, 0)[...]
        for d in range(1, n_y):
            y_copy(k, d).wait_recv()
            total = total + yrecv[k, d - 1].astype(F32)

        @pl.when(k >= 2)
        def _():
            out_copy(k - 2).wait()

        obuf[k % 2] = total.astype(BF16)
        out_copy(k).start()

    def out_step(k, _):
        for i in range(n_sp):
            @pl.when(k == i)
            def _():
                j = (i + 1) // 2
                if i == 0:
                    ring.tick(done_in + 0.28)
                elif j < hops:
                    ring.need(("out", 0, 0, j))
                    ring.need(("out", 1, 0, j))
                else:
                    ring.need(("out", 0, 0, j))

        stage_one(k)
        stage_two(k)

        @pl.when(k >= 1)
        def _():
            stage_three(k - 1)

        return 0

    lax.fori_loop(0, n_sp, out_step, 0)
    stage_three(n_sp - 1)
    ring.close()
    for k in range(max(0, n_sp - 2), n_sp):
        core_copy(k).wait_send()
        out_copy(k).wait()

    def drain(k, _):
        for d in range(1, n_y):
            y_copy(k, d).wait_send()
        return 0

    lax.fori_loop(0, n_sp, drain, 0)

    halo_leave(POOL)
    for r in range(n_round):
        @pl.when(sp + shifts[r] < n_sp)
        def _():
            scan_copy(r, sources[r]).wait_send()


def pool_mix(cfg, raw, gmw, cscale_ref, sp, tp, tile, rows, width):
    groups = gmw.shape[0]

    def body(t, _):
        window = pl.ds(pl.multiple_of(t * tile, tile), tile + PAD)
        to = pl.ds(pl.multiple_of(PAD + t * tile, PAD), tile)
        place = sp * rows + t * tile + lax.broadcasted_iota(jnp.int32, (tile, 1), 0) + 1
        for g in range(groups):
            cols = slice(g * GROUP_DIM, (g + 1) * GROUP_DIM)
            extended = raw[POOL, window, cols].astype(F32)
            sums = extended
            options = []
            for lag in (1, 2, 4, 8):
                sums = sums + pltpu.roll(sums, lag, 0)
                options.append(sums[PAD:])
            if groups % 4 == 0:
                size = 2 << (g % 4)
                windowed = options[g % 4]
            else:
                which = (tp * groups + g) % 4
                size = jnp.where(which == 0, 2, jnp.where(which == 1, 4, jnp.where(which == 2, 8, 16)))
                windowed = options[3]
                for i in range(3):
                    windowed = jnp.where(which == i, options[i], windowed)
            counts = jnp.minimum(place, size).astype(F32)
            diff = (windowed / counts - extended[PAD:]).astype(BF16)
            mixed = jnp.dot(diff, gmw[g], preferred_element_type=F32)
            scale = cscale_ref[:, pl.ds(pl.multiple_of(tp * width + g * GROUP_DIM, 128), GROUP_DIM)]
            raw[KEY, to, cols] = (mixed * scale.astype(F32)).astype(BF16)
        return 0

    lax.fori_loop(0, rows // tile, body, 0)


def per_device(
    n_sp,
    n_tp,
    tokens,
    input_norm_scale,
    mean_input_weight,
    query_matrix,
    key_matrix,
    value_matrix,
    strength_weight,
    decay_input_weight,
    causal_filter_weight,
    head_decay_logrates,
    decay_input_shift,
    strength_shift,
    decay_spike,
    head_norm_scale,
    group_mixing_weight,
    mean_channel_scale,
    mean_output_weight,
    delta_output_weight,
):
    rows, dim = tokens.shape
    rows_in, width = key_matrix.shape
    heads = strength_weight.shape[1]
    depth = width // heads
    rows_out, cols_out = mean_output_weight.shape
    n_y = n_tp // 2
    share = rows // n_tp
    groups = mean_input_weight.shape[1] // GROUP_DIM
    hops = n_sp // 2
    grid_x = 1
    while grid_x * grid_x * 4 <= n_sp:
        grid_x *= 2
    narrow = jnp.concatenate([strength_weight, decay_input_weight], axis=1).T
    narrow = jnp.pad(narrow, ((0, PAD - 2 * heads), (0, width - rows_in)))
    n_items = 3 * hops + 2 * (2 * hops - 1)
    n_round = 2
    while 2 ** (n_round - 1) < n_sp - 1:
        n_round += 1
    any_ = pl.BlockSpec(memory_space=pl.ANY)
    vmem = pl.BlockSpec(memory_space=pltpu.VMEM)
    dma = pltpu.SemaphoreType.DMA
    return pl.pallas_call(
        lambda *refs: mixer_kernel((n_sp, n_tp, heads, depth, grid_x), *refs),
        out_shape=jax.ShapeDtypeStruct((share, dim), BF16),
        in_specs=[any_, vmem, any_, any_, any_, any_, any_]
        + [vmem] * 6
        + [any_, vmem, any_, any_],
        out_specs=any_,
        scratch_shapes=[
            pltpu.VMEM((4, n_sp, rows_in + PAD, width), BF16),
            pltpu.VMEM((2, n_sp, rows_out, cols_out), BF16),
            pltpu.VMEM((n_sp, rows, rows_in), BF16),
            pltpu.VMEM((4, rows, width), F32),
            pltpu.VMEM((4, rows + PAD, width), BF16),
            pltpu.VMEM((2, min(128, rows), dim), BF16),
            pltpu.VMEM((rows, PAD), F32),
            pltpu.VMEM((groups, GROUP_DIM, GROUP_DIM), BF16),
            pltpu.VMEM((heads, depth, 2 * depth), F32),
            pltpu.VMEM((n_round, heads, depth, 2 * depth), BF16),
            pltpu.VMEM((n_round, heads, depth, 2 * depth), BF16),
            pltpu.VMEM((2, n_y, share, cols_out), BF16),
            pltpu.VMEM((n_sp, n_y, share, cols_out), BF16),
            pltpu.VMEM((n_sp, n_y - 1, share, cols_out), BF16),
            pltpu.VMEM((n_sp, n_y - 1, share, cols_out), BF16),
            pltpu.VMEM((2, share, cols_out), BF16),
            dma((n_items, 2)),
            dma((n_items, 2)),
            dma((8,)),
            dma((2,)),
            dma((4,)),
            dma((4,)),
            dma((n_round,)),
            dma((n_round,)),
            dma((n_sp,)),
            dma((n_sp,)),
            dma((n_sp, n_y - 1)),
            dma((n_sp, n_y - 1)),
            dma((2,)),
        ],
        compiler_params=pltpu.CompilerParams(
            collective_id=0, has_side_effects=True, vmem_limit_bytes=67043328
        ),
    )(
        tokens,
        input_norm_scale.reshape(1, dim),
        key_matrix,
        value_matrix,
        query_matrix,
        mean_input_weight,
        narrow,
        causal_filter_weight,
        head_decay_logrates.reshape(1, -1),
        decay_input_shift.reshape(1, -1),
        strength_shift.reshape(1, -1),
        decay_spike,
        head_norm_scale.reshape(1, -1),
        group_mixing_weight,
        mean_channel_scale.reshape(1, -1),
        mean_output_weight,
        delta_output_weight,
    )


def solution(mesh):
    n_sp, n_tp = mesh.shape["sp"], mesh.shape["tp"]
    return jax.shard_map(
        lambda *args: per_device(n_sp, n_tp, *args),
        mesh=mesh,
        in_specs=(
            P("sp", None),
            P(),
            P("sp", "tp"),
            P("sp", "tp"),
            P("sp", "tp"),
            P("sp", "tp"),
            P("sp", "tp"),
            P("sp", "tp"),
            P(),
            P(),
            P(),
            P(),
            P("sp", "tp"),
            P(),
            P(),
            P(),
            P("tp", "sp"),
            P("tp", "sp"),
        ),
        out_specs=P(("sp", "tp"), None),
        check_vma=False,
    )
```

```python
import jax
import jax.numpy as jnp
from jax import lax
from jax.experimental import pallas as pl
from jax.experimental.pallas import tpu as pltpu
from jax.sharding import PartitionSpec as P

GROUP_DIM = 128
CONV = 4
EPSILON = 1e-06
PAD = 16
CHUNK = 128
BF16 = jnp.bfloat16
F32 = jnp.float32
MESH = pl.DeviceIdType.MESH
STATE_PART = 0.12
LAST_SINGLE = 2
MIDDLE = 2
SPLIT = 2
QUERY_PART = 0.03
KEY, VAL, QRY, POOL = range(4)


def dot(left, right):
    return jnp.dot(left.astype(BF16), right.astype(BF16), preferred_element_type=F32)


def dot_nt(left, right):
    return lax.dot_general(
        left.astype(BF16),
        right.astype(BF16),
        (((1,), (1,)), ((), ())),
        preferred_element_type=F32,
    )


def dot_tn(left, right):
    return lax.dot_general(
        left.astype(BF16),
        right.astype(BF16),
        (((0,), (0,)), ((), ())),
        preferred_element_type=F32,
    )


def unit_rows(values):
    return values * lax.rsqrt(jnp.sum(values * values, axis=-1, keepdims=True) + EPSILON)


def convolve(extended, taps, chunk):
    extended = extended.astype(F32)
    total = jnp.zeros((chunk, extended.shape[1]), F32)
    for i in range(CONV):
        start = PAD - (CONV - 1) + i
        total = total + taps[i] * extended[start : start + chunk]
    return total / (1.0 + jnp.exp(-total))


def decay_weights(cum_cols, cum_rows, h, causal):
    spread = cum_cols[:, h : h + 1] - cum_rows[h : h + 1, :]
    return jnp.where(causal, jnp.exp(jnp.where(causal, spread, 0.0)), 0.0)


def state_chunk(heads, depth, chunk, convolved, beta, decay, carry):
    row = lax.broadcasted_iota(jnp.int32, (chunk, chunk), 0)
    col = lax.broadcasted_iota(jnp.int32, (chunk, chunk), 1)
    causal = row >= col
    strict = row > col
    eye = jnp.where(row == col, 1.0, 0.0)
    tri = jnp.where(causal, 1.0, 0.0)
    cum_cols = jnp.dot(tri, decay, preferred_element_type=F32, precision=lax.Precision.HIGHEST)
    cum_rows = lax.dot_general(
        decay,
        tri,
        (((0,), (1,)), ((), ())),
        preferred_element_type=F32,
        precision=lax.Precision.HIGHEST,
    )
    base = min(16, chunk)
    hs = range(heads)
    k = [unit_rows(convolved[0][:, h * depth : (h + 1) * depth]) for h in hs]
    v = [convolved[1][:, h * depth : (h + 1) * depth] for h in hs]
    cum = [cum_cols[:, h : h + 1] for h in hs]
    last = [cum_cols[chunk - 1 : chunk, h : h + 1] for h in hs]
    beta = [beta[:, h : h + 1] for h in hs]
    weights = [decay_weights(cum_cols, cum_rows, h, causal) for h in hs]
    kb = [k[h] * beta[h] for h in hs]
    lower = [jnp.where(strict, dot_nt(kb[h], k[h]) * weights[h], 0.0) for h in hs]
    power = [jnp.where(row // base == col // base, lower[h], 0.0) for h in hs]
    inverse = [eye - power[h] for h in hs]
    reach = 2
    while reach < base:
        power = [dot(power[h], power[h]) for h in hs]
        inverse = [inverse[h] + dot(inverse[h], power[h]) for h in hs]
        reach *= 2
    size = base
    while size < chunk:
        pair = (row // (2 * size) == col // (2 * size)) & (row // size != col // size)
        right = [dot(jnp.where(pair, lower[h], 0.0), inverse[h]) for h in hs]
        inverse = [inverse[h] - dot(inverse[h], right[h]) for h in hs]
        size *= 2
    grow = [jnp.exp(cum[h]) for h in hs]
    sides = [jnp.concatenate([v[h] * beta[h], kb[h] * grow[h]], axis=1) for h in hs]
    solved = [dot(inverse[h], sides[h]) for h in hs]
    kd = [k[h] * jnp.exp(last[h] - cum[h]) for h in hs]
    zeros = jnp.zeros((chunk, depth), F32)
    state = [carry[h] for h in hs]
    fresh = [
        jnp.concatenate([solved[h][:, :depth], zeros], axis=1) - dot(solved[h][:, depth:], state[h])
        for h in hs
    ]
    for h in hs:
        carry[h] = state[h] * jnp.exp(last[h]) + dot_tn(kd[h], fresh[h])
    return k, cum_cols, cum_rows, state, fresh


class Ring:
    def __init__(self, hops, split, half_rows, refs, sems, owner, peers, window):
        self.refs, self.sems, self.owner, self.peers, self.window = refs, sems, owner, peers, window
        self.items = []
        self.index = {}
        rows_in, rows_out = half_rows
        top = rows_in // 2
        for j in range(1, hops + 1):
            for m in (KEY, VAL):
                full = rows_in + PAD if m == KEY else rows_in
                if j < hops:
                    self.add(("in", m, 0), j, [("in", m, 0, full)] * 2)
                else:
                    self.add(("in", m, 0), j, [("in", m, 0, top), ("in", m, top, full)])
        for j in range(1, hops + 1):
            for m in (QRY, POOL):
                if j < hops:
                    self.add(("in", m, 0), j, [("in", m, 0, top)] * 2)
                    self.add(("in", m, 1), j, [("in", m, top, rows_in)] * 2)
                else:
                    self.add(("in", m, 0), j, [("in", m, 0, top), ("in", m, top, rows_in)])
        for j in range(1, hops + 1):
            for e in range(split if j < hops else split // 2):
                other = e if j < hops else split // 2 + e
                self.add(("out", e, 0), j, [("out", e, 0, rows_out), ("out", other, 0, rows_out)])
        self.finish = []
        total = 0
        for _, _, parts in self.items:
            total += (parts[0][3] - parts[0][2]) * refs[parts[0][0]].shape[3]
            self.finish.append(total)
        self.total = total
        self.started = 0
        self.sent = set()
        self.received = set()

    def add(self, key, j, parts):
        self.index[key + (j,)] = len(self.items)
        self.items.append((key, j, parts))

    def copy(self, i, side):
        key, j, parts = self.items[i]
        kind, m, low, high = parts[side]
        ref = self.refs[kind]
        block = ref.at[m, self.owner(-(j - 1) if side == 0 else j - 1), pl.ds(low, high - low), :]
        return pltpu.make_async_remote_copy(
            src_ref=block,
            dst_ref=block,
            send_sem=self.sems[0].at[i, side],
            recv_sem=self.sems[1].at[i, side],
            device_id=self.peers[side],
            device_id_type=MESH,
        )

    def arrive(self, i, side):
        if (i, side) in self.received:
            return
        self.received.add((i, side))
        self.copy(i, side).wait_recv()

    def leave(self, i):
        if i in self.sent:
            return
        self.sent.add(i)
        for side in range(2):
            self.copy(i, side).wait_send()

    def start_next(self):
        i = self.started
        if i >= len(self.items):
            return
        behind = i - self.ahead(i)
        if behind >= 0:
            self.leave(behind)
        key, j, parts = self.items[i]
        for side in range(2):
            if j > 1:
                kind, m, low, high = parts[side]
                for before in range(i):
                    other, hop, pieces = self.items[before]
                    if hop == j - 1 and pieces[side][:2] == (kind, m) and pieces[side][2] <= low < pieces[side][3]:
                        self.arrive(before, side)
                    elif hop == j - 1 and pieces[side][:2] == (kind, m) and low <= pieces[side][2] < high:
                        self.arrive(before, side)
            self.copy(i, side).start()
        self.started += 1

    def ahead(self, i):
        if i >= len(self.items) - LAST_SINGLE:
            return 1
        return MIDDLE if self.items[i][0][1] in (QRY, POOL) and self.items[i][0][0] == "in" else 2

    def tick(self, part):
        while self.started < len(self.items):
            behind = self.started - self.ahead(self.started)
            if behind >= 0 and self.finish[behind] > part * self.total:
                break
            self.start_next()

    def need(self, key):
        i = self.index[key]
        while self.started < len(self.items) and self.started - self.ahead(self.started) <= i:
            self.start_next()
        for side in range(2):
            self.arrive(i, side)

    def close(self):
        while self.started < len(self.items):
            self.start_next()
        for i in range(len(self.items)):
            for side in range(2):
                self.arrive(i, side)
            self.leave(i)


def mixer_kernel(cfg, *refs):
    (
        tok_ref, gain_ref, wk_ref, wv_ref, wq_ref, wp_ref, strength_ref, slow_ref, tap_ref, rate_ref,
        dshift_ref, sshift_ref, spike_ref, hgain_ref, gmw_ref, cscale_ref, wpo_ref, wdo_ref,
    ) = refs[:18]
    out_ref = refs[18]
    (
        win, wout, normed, acc, raw, stage, before_tok, nraw, rowcum, tail, gain, cscale, gmw, carry, held,
        caught, psend, corerecv, ysend, yrecv, obuf, ring_send, ring_recv, local_sem, tok_sem, halo_sem,
        scan_send, scan_recv, core_send, core_recv, y_send, y_recv, out_sem,
    ) = refs[19:]
    n_sp, n_tp, heads, depth, grid_x = cfg
    grid_z = n_sp // grid_x
    hops = n_sp // 2
    n_y = n_tp // 2
    rows, width = raw.shape[1] - PAD, raw.shape[2]
    rows_in = normed.shape[2]
    split, rows_out, cols_half = wout.shape[0], wout.shape[2] // 2, wout.shape[3]
    share = rows // n_tp
    sp = lax.axis_index("sp")
    tp = lax.axis_index("tp")
    core = tp % 2
    ypos = tp // 2

    def sp_at(r):
        s = jnp.maximum(r - grid_z, 0)
        i = s // (grid_x - 1)
        k = s % (grid_x - 1)
        x = 1 + jnp.where(i % 2 == 0, k, grid_x - 2 - k)
        return jnp.where(r < grid_z, r * grid_x, (grid_z - 1 - i) * grid_x + x)

    zc = sp // grid_x
    xc = sp % grid_x
    ic = grid_z - 1 - zc
    kc = jnp.where(ic % 2 == 0, xc - 1, grid_x - 1 - xc)
    pos = jnp.where(xc == 0, zc, grid_z + ic * (grid_x - 1) + kc)

    def owner(offset):
        return sp_at((pos + offset + n_sp) % n_sp)

    barrier = pltpu.get_barrier_semaphore()
    for k in range(1, n_sp):
        pl.semaphore_signal(barrier, inc=1, device_id=((sp + k) % n_sp, tp), device_id_type=MESH)
    for k in range(1, n_tp):
        pl.semaphore_signal(barrier, inc=1, device_id=(sp, (tp + k) % n_tp), device_id_type=MESH)

    locals_ = []

    def bring(src, dst):
        locals_.append(pltpu.make_async_copy(src, dst, local_sem.at[len(locals_)]))
        locals_[-1].start()

    groups = gmw.shape[0]
    bring(wk_ref, win.at[KEY, sp, pl.ds(0, rows_in), :])
    bring(wv_ref, win.at[VAL, sp, pl.ds(0, rows_in), :])
    bring(wq_ref, win.at[QRY, sp, pl.ds(0, rows_in), :])
    bring(wp_ref, win.at[POOL, sp, pl.ds(0, rows_in), :])
    for half in range(split):
        cols = pl.ds(half * cols_half, cols_half)
        bring(wpo_ref.at[:, cols], wout.at[half, sp, pl.ds(0, rows_out), :])
        bring(wdo_ref.at[:, cols], wout.at[half, sp, pl.ds(rows_out, rows_out), :])
    bring(gmw_ref.at[pl.ds(tp * groups, groups)], gmw)
    step_rows = stage.shape[1]
    n_stage = rows // step_rows

    def token_copy(t, slot):
        return pltpu.make_async_copy(
            tok_ref.at[pl.ds(pl.multiple_of(t * step_rows, step_rows), step_rows), :],
            stage.at[slot],
            tok_sem.at[slot],
        )

    token_copy(0, 0).start()
    win[KEY, sp, pl.ds(rows_in, PAD), pl.ds(0, rows_in)] = jnp.concatenate(
        [
            strength_ref[...].astype(F32),
            slow_ref[...].astype(F32),
            jnp.zeros((PAD - 2 * heads, rows_in), F32),
        ],
        axis=0,
    ).astype(BF16)
    for i in range(gain_ref.shape[0]):
        gain[:, i * 128 : (i + 1) * 128] = gain_ref[i : i + 1, :].astype(F32)
    cscale[...] = cscale_ref[...].astype(F32)
    locals_[0].wait()
    locals_[1].wait()
    pl.semaphore_wait(barrier, n_sp + n_tp - 2)

    halo = pltpu.make_async_remote_copy(
        src_ref=tok_ref.at[pl.ds(rows - PAD, PAD), :],
        dst_ref=before_tok,
        send_sem=halo_sem.at[0],
        recv_sem=halo_sem.at[1],
        device_id=((sp + 1) % n_sp, tp),
        device_id_type=MESH,
    )

    @pl.when(sp + 1 < n_sp)
    def _():
        halo.start()

    ring = Ring(
        hops,
        split,
        (rows_in, wout.shape[2]),
        {"in": win, "out": wout},
        (ring_send, ring_recv),
        owner,
        [(owner(1), tp), (owner(-1), tp)],
        2,
    )
    ring.tick(0.0)
    for c in locals_[2:]:
        c.wait()

    def norm_rows(load, to, count):
        squares = jnp.zeros((count, 1), F32)
        for b in range(n_sp):
            x = load(slice(b * rows_in, (b + 1) * rows_in)).astype(F32)
            squares = squares + jnp.sum(x * x, axis=-1, keepdims=True)
        scale = lax.rsqrt(squares * (1.0 / (n_sp * rows_in)) + EPSILON)
        for b in range(n_sp):
            cols = slice(b * rows_in, (b + 1) * rows_in)
            normed[b, to, :] = (load(cols).astype(F32) * scale * gain[:, cols]).astype(BF16)

    def norm_step(t, _):
        slot = t % 2
        token_copy(t, slot).wait()

        @pl.when(t + 1 < n_stage)
        def _():
            token_copy(t + 1, 1 - slot).start()

        def piece(u, _):
            at = pl.ds(pl.multiple_of(u * 32, 32), 32)
            to = pl.ds(pl.multiple_of(PAD + t * step_rows + u * 32, PAD), 32)
            norm_rows(lambda cols: stage[slot, at, cols], to, 32)
            return 0

        lax.fori_loop(0, step_rows // 32, piece, 0)
        return 0

    lax.fori_loop(0, n_stage, norm_step, 0)

    @pl.when(sp > 0)
    def _():
        halo.wait_recv()

    @pl.when(sp == 0)
    def _():
        before_tok[...] = jnp.zeros(before_tok.shape, BF16)

    norm_rows(lambda cols: before_tok[:, cols], pl.ds(0, PAD), PAD)

    tile = max(d for d in range(PAD, 273, PAD) if (rows + PAD) % d == 0)
    n_tile = (rows + PAD) // tile

    def project(m, owners, first=False, final=False):
        def body(t, _):
            at = pl.ds(pl.multiple_of(t * tile, PAD), tile)
            total = None if first else acc[m, at, :]
            for o in owners:
                term = jnp.dot(
                    normed[o, at, :], win[m, o, pl.ds(0, rows_in), :], preferred_element_type=F32
                )
                total = term if total is None else total + term
            if final:
                raw[m, at, :] = total.astype(BF16)
            else:
                acc[m, at, :] = total
            return 0

        lax.fori_loop(0, n_tile, body, 0)

    def own(m, _):
        project(m, [sp], first=True)
        return 0

    lax.fori_loop(0, 4, own, 0)

    def arriving(i, _):
        for k in range(2 * hops):
            @pl.when(i == k)
            def _():
                ring.need(("in", k % 2, 0, k // 2 + 1))

        m, j = i % 2, i // 2 + 1

        @pl.when(j < hops)
        def _():
            project(m, [owner(-j), owner(j)])

        @pl.when(j == hops)
        def _():
            project(m, [owner(hops)], final=True)

        return 0

    lax.fori_loop(0, 2 * hops, arriving, 0)
    block = min(256, rows)
    n_block = rows // block

    def narrow_body(t, _):
        at = pl.ds(pl.multiple_of(t * block, block), block)
        total = jnp.zeros((block, PAD), F32)
        for o in range(n_sp):
            total = total + dot_nt(
                normed[o, pl.ds(pl.multiple_of(PAD + t * block, PAD), block), :],
                win[KEY, o, pl.ds(rows_in, PAD), pl.ds(0, rows_in)],
            )
        nraw[at, :] = total
        return 0

    lax.fori_loop(0, n_block, narrow_body, 0)

    lane = lax.broadcasted_iota(jnp.int32, (1, rate_ref.shape[1]), 1)
    small = lax.broadcasted_iota(jnp.int32, (1, heads), 1)

    def head_row(ref):
        total = jnp.zeros((1, heads), F32)
        for h in range(heads):
            value = jnp.sum(jnp.where(lane == tp * heads + h, ref[...], 0.0), axis=-1, keepdims=True)
            total = total + jnp.where(small == h, value, 0.0)
        return total

    speed = -jnp.exp(head_row(rate_ref))
    dshift = head_row(dshift_ref)
    sshift = head_row(sshift_ref)
    mine = pl.ds(pl.multiple_of(tp * width, 128), width)
    wide = lax.broadcasted_iota(jnp.int32, (depth, 2 * depth), 1)
    sub = lax.broadcasted_iota(jnp.int32, (depth, 2 * depth), 0)
    for h in range(heads):
        carry[h] = jnp.where(wide == sub + depth, 1.0, 0.0)
    chunk = min(CHUNK, rows)
    n_chunk = rows // chunk
    tail[...] = raw[KEY, pl.ds(0, PAD), :]
    one = lax.broadcasted_iota(jnp.int32, (heads, heads), 0) == lax.broadcasted_iota(
        jnp.int32, (heads, heads), 1
    )
    per_slot = stage.shape[2] // (2 * depth)
    fresh_at = [((h * 2 * depth) // width, (h * 2 * depth) % width) for h in range(heads)]

    def stage_at(c, h):
        flat = c * heads + h
        cols = pl.ds(pl.multiple_of((flat % per_slot) * 2 * depth, 128), 2 * depth)
        return stage.at[flat // per_slot, pl.ds(0, depth), cols]

    third = 1.0 / 3.0

    def state_step(c, _):
        for k in range(n_chunk):
            @pl.when(c == k)
            def _():
                ring.tick(third + STATE_PART * k / n_chunk)

        at = pl.ds(pl.multiple_of(c * chunk, chunk), chunk)
        to = pl.ds(pl.multiple_of(PAD + c * chunk, PAD), chunk)
        window = pl.ds(pl.multiple_of(c * chunk, chunk), chunk + PAD)
        keys = jnp.concatenate([tail[...], raw[KEY, to, :]], axis=0)
        tail[...] = keys[chunk:]
        taps = [[tap_ref[r, i : i + 1, mine].astype(F32) for i in range(CONV)] for r in range(3)]
        convolved = [convolve(keys, taps[1], chunk), convolve(raw[VAL, window, :], taps[2], chunk)]
        narrow = nraw[at, :].astype(BF16).astype(F32)
        beta = 1.0 / (1.0 + jnp.exp(-(narrow[:, :heads] + sshift)))
        x = narrow[:, heads : 2 * heads] + dshift
        soft = jnp.maximum(x, 0.0) + jnp.log1p(jnp.exp(-jnp.abs(x)))
        spike = lax.dot_general(
            spike_ref[:, at],
            jnp.where(one, 1.0, 0.0),
            (((0,), (0,)), ((), ())),
            preferred_element_type=F32,
            precision=lax.Precision.HIGHEST,
        )
        decay = speed * soft + spike
        k, cum_cols, cum_rows, state, fresh = state_chunk(
            heads, depth, chunk, convolved, beta, decay, carry
        )
        nraw[at, pl.ds(0, heads)] = cum_cols
        rowcum[c] = cum_rows
        for h in range(heads):
            raw[KEY, to, h * depth : (h + 1) * depth] = k[h].astype(BF16)
            stage_at(c, h)[...] = state[h].astype(BF16)
            slot, low = fresh_at[h]
            acc[slot, at, low : low + 2 * depth] = fresh[h]
        return 0

    lax.fori_loop(0, n_chunk, state_step, 0)

    far = grid_x - 1
    whole, front = pl.ds(0, 2 * depth), pl.ds(0, depth)

    def pass_state(slot, source, target, pick, z, x):
        return pltpu.make_async_remote_copy(
            src_ref=source.at[:, :, pick],
            dst_ref=caught.at[target, :, :, pick],
            send_sem=scan_send.at[slot],
            recv_sem=scan_recv.at[target],
            device_id=(z * grid_x + x, tp),
            device_id_type=MESH,
        )

    along_x = pass_state(0, held.at[0], 0, whole, zc, (xc + 1) % grid_x)
    along_z = pass_state(1, held.at[1], 1, front, (zc + 1) % grid_z, xc)
    back = [
        pass_state(2 + x, caught.at[1], 2, front, zc, (xc + 1 + x) % grid_x) for x in range(far)
    ]

    @pl.when(xc == 0)
    def _():
        for h in range(heads):
            held[0, h] = carry[h].astype(BF16)
            caught[0, h] = jnp.where(wide == sub + depth, 1.0, 0.0).astype(BF16)
        along_x.start()

    def x_stage(x):
        @pl.when(xc == x)
        def _():
            along_x.wait_recv()
            for h in range(heads):
                later = carry[h]
                pushed = dot(later[:, depth:], caught[0, h])
                held[0, h, :, front] = (later[:, :depth] + pushed[:, :depth]).astype(BF16)
                held[0, h, :, pl.ds(depth, depth)] = pushed[:, depth:].astype(BF16)
            if x < far:
                along_x.start()

    def z_stage(z):
        @pl.when((xc == far) & (zc == z))
        def _():
            if z == 0:
                for h in range(heads):
                    caught[1, h, :, front] = jnp.zeros((depth, depth), BF16)
            else:
                along_z.wait_recv()
                for c in back:
                    c.start()
            if z + 1 < grid_z:
                for h in range(heads):
                    later = held[0, h]
                    pushed = dot(later[:, depth:], caught[1, h, :, front])
                    held[1, h, :, front] = (later[:, :depth].astype(F32) + pushed).astype(BF16)
                along_z.start()

    def last_stage():
        @pl.when((xc < far) & (zc > 0))
        def _():
            back[0].wait_recv()
            for h in range(heads):
                caught[1, h, :, front] = caught[2, h, :, front]

        @pl.when((xc < far) & (zc == 0))
        def _():
            for h in range(heads):
                caught[1, h, :, front] = jnp.zeros((depth, depth), BF16)

        for h in range(heads):
            later = caught[0, h]
            pushed = dot(later[:, depth:], caught[1, h, :, front])
            held[2, h, :, front] = (later[:, :depth].astype(F32) + pushed).astype(BF16)

    incoming = held.at[2]

    def hop(m, j):
        ring.need(("in", m, 0, j))
        if j < hops:
            ring.need(("in", m, 1, j))
            project(m, [owner(-j), owner(j)])
        else:
            project(m, [owner(hops)], final=True)

    steps = [(m, j) for j in range(1, hops + 1) for m in (QRY, POOL)][:-1]
    for i, (m, j) in enumerate(steps):
        hop(m, j)
        if 2 <= i <= far + 1:
            x_stage(i - 1)
        if far < i <= far + grid_z:
            z_stage(i - far - 1)
    last_stage()

    hgain = hgain_ref[...].astype(F32)
    row = lax.broadcasted_iota(jnp.int32, (chunk, chunk), 0)
    col = lax.broadcasted_iota(jnp.int32, (chunk, chunk), 1)
    causal = row >= col

    def query_step(c, _):
        for k in range(n_chunk):
            @pl.when(c == k)
            def _():
                ring.tick(2 * third - 0.02 + QUERY_PART * k / n_chunk)

        at = pl.ds(pl.multiple_of(c * chunk, chunk), chunk)
        to = pl.ds(pl.multiple_of(PAD + c * chunk, PAD), chunk)
        window = pl.ds(pl.multiple_of(c * chunk, chunk), chunk + PAD)
        taps = [tap_ref[0, i : i + 1, mine].astype(F32) for i in range(CONV)]
        convolved = convolve(raw[QRY, window, :], taps, chunk)
        cum_cols = nraw[at, :]
        cum_rows = rowcum[c]
        hs = range(heads)
        spans = [slice(h * depth, (h + 1) * depth) for h in hs]
        q = [unit_rows(convolved[:, spans[h]]) * depth ** (-0.5) for h in hs]
        weights = [decay_weights(cum_cols, cum_rows, h, causal) for h in hs]
        scores = [dot_nt(q[h], raw[KEY, to, spans[h]]) * weights[h] for h in hs]
        grow = [jnp.exp(cum_cols[:, h : h + 1]) for h in hs]
        outs = []
        for h in hs:
            slot, low = fresh_at[h]
            outs.append(
                dot(q[h] * grow[h], stage_at(c, h)[...])
                + dot(scores[h], acc[slot, at, low : low + 2 * depth])
            )
        values = [
            outs[h][:, :depth] + dot(outs[h][:, depth:], incoming[h, :, pl.ds(0, depth)]) for h in hs
        ]
        for h in hs:
            scale = lax.rsqrt(jnp.mean(values[h] * values[h], axis=-1, keepdims=True) + EPSILON)
            raw[VAL, to, spans[h]] = (values[h] * scale * hgain).astype(BF16)
        return 0

    lax.fori_loop(0, n_chunk, query_step, 0)
    hop(POOL, hops)
    pool_mix(cfg, raw, gmw, cscale, sp, tp, block, rows, width)

    n_pair = split * hops

    def half_of(p, u):
        q = jnp.maximum(p - split // 2, 0)
        t = p - (n_pair - split // 2)
        step = jnp.where(p < split // 2, 0, q // split + 1)
        part = jnp.where(
            p < split // 2, 2 * p + u, jnp.where(t >= 0, u * (split // 2) + t, q % split)
        )
        return owner((2 * u - 1) * step), part

    def partial(dest, o, half):
        at = pl.ds(pl.multiple_of(PAD + dest * share, PAD), share)
        total = jnp.dot(
            raw[KEY, at, :], wout[half, o, pl.ds(0, rows_out), :], preferred_element_type=F32
        ) + jnp.dot(
            raw[VAL, at, :], wout[half, o, pl.ds(rows_out, rows_out), :], preferred_element_type=F32
        )
        return total.astype(BF16)

    def core_copy(p):
        return pltpu.make_async_remote_copy(
            src_ref=psend.at[p % 2],
            dst_ref=corerecv.at[p],
            send_sem=core_send.at[p],
            recv_sem=core_recv.at[p],
            device_id=(sp, ypos * 2 + 1 - core),
            device_id_type=MESH,
        )

    def y_copy(p, d):
        return pltpu.make_async_remote_copy(
            src_ref=ysend.at[p, d - 1],
            dst_ref=yrecv.at[p, d - 1],
            send_sem=y_send.at[p, d - 1],
            recv_sem=y_recv.at[p, d - 1],
            device_id=(sp, ((ypos + d) % n_y) * 2 + core),
            device_id_type=MESH,
        )

    def out_copy(p, u):
        o, half = half_of(p, u)
        low = (o * split + half) * cols_half
        return pltpu.make_async_copy(
            obuf.at[p % 2, u],
            out_ref.at[:, pl.ds(pl.multiple_of(low, 128), cols_half)],
            out_sem.at[p % 2, u],
        )

    def own_at(p, u):
        at = pl.ds(pl.multiple_of((p % 4) * share, share), share)
        return acc.at[QRY, at, pl.ds(u * cols_half, cols_half)]

    def stage_one(p):
        @pl.when(p >= 2)
        def _():
            core_copy(p - 2).wait_send()

        for u in range(2):
            o, half = half_of(p, u)
            for y in range(n_y):
                psend[p % 2, y, u] = partial(y * 2 + 1 - core, o, half)
        core_copy(p).start()

    def stage_two(p):
        parts = []
        for u in range(2):
            o, half = half_of(p, u)
            parts.append([partial(((ypos + d) % n_y) * 2 + core, o, half) for d in range(n_y)])
        core_copy(p).wait_recv()
        for d in range(1, n_y):
            there = (ypos + d) % n_y
            for u in range(2):
                total = parts[u][d].astype(F32) + corerecv[p, there, u].astype(F32)
                ysend[p, d - 1, u] = total.astype(BF16)
            y_copy(p, d).start()
        for u in range(2):
            own_at(p, u)[...] = parts[u][0].astype(F32) + corerecv[p, ypos, u].astype(F32)

    def stage_three(p):
        for d in range(1, n_y):
            y_copy(p, d).wait_recv()
        for u in range(2):
            total = own_at(p, u)[...]
            for d in range(1, n_y):
                total = total + yrecv[p, d - 1, u].astype(F32)

            @pl.when(p >= 2)
            def _():
                out_copy(p - 2, u).wait()

            obuf[p % 2, u] = total.astype(BF16)
            out_copy(p, u).start()

    def out_step(p, _):
        for i in range(n_pair):
            @pl.when(p == i)
            def _():
                if i < split // 2:
                    ring.tick(2 * third)
                else:
                    e = i - split // 2
                    ring.need(("out", e % split, 0, e // split + 1))

        stage_one(p)

        @pl.when(p >= 2)
        def _():
            stage_three(p - 2)

        stage_two(p)
        return 0

    lax.fori_loop(0, n_pair, out_step, 0)
    stage_three(n_pair - 2)
    stage_three(n_pair - 1)
    ring.close()
    for p in range(n_pair - 2, n_pair):
        core_copy(p).wait_send()
        for u in range(2):
            out_copy(p, u).wait()

    def drain(p, _):
        for d in range(1, n_y):
            y_copy(p, d).wait_send()
        return 0

    lax.fori_loop(0, n_pair, drain, 0)

    @pl.when(sp + 1 < n_sp)
    def _():
        halo.wait_send()

    @pl.when(xc < far)
    def _():
        along_x.wait_send()

    @pl.when((xc == far) & (zc + 1 < grid_z))
    def _():
        along_z.wait_send()

    @pl.when((xc == far) & (zc > 0))
    def _():
        for c in back:
            c.wait_send()


def pool_mix(cfg, raw, gmw, cscale, sp, tp, tile, rows, width):
    groups = gmw.shape[0]

    def body(t, _):
        window = pl.ds(pl.multiple_of(t * tile, tile), tile + PAD)
        to = pl.ds(pl.multiple_of(PAD + t * tile, PAD), tile)
        place = sp * rows + t * tile + lax.broadcasted_iota(jnp.int32, (tile, 1), 0) + 1
        for g in range(groups):
            cols = slice(g * GROUP_DIM, (g + 1) * GROUP_DIM)
            extended = raw[POOL, window, cols].astype(F32)
            sums = extended
            options = []
            for lag in (1, 2, 4, 8):
                sums = sums + pltpu.roll(sums, lag, 0)
                options.append(sums[PAD:])
            if groups % 4 == 0:
                size = 2 << (g % 4)
                windowed = options[g % 4]
            else:
                which = (tp * groups + g) % 4
                size = jnp.where(which == 0, 2, jnp.where(which == 1, 4, jnp.where(which == 2, 8, 16)))
                windowed = options[3]
                for i in range(3):
                    windowed = jnp.where(which == i, options[i], windowed)
            counts = jnp.minimum(place, size).astype(F32)
            diff = (windowed / counts - extended[PAD:]).astype(BF16)
            mixed = jnp.dot(diff, gmw[g], preferred_element_type=F32)
            scale = cscale[pl.ds(tp * groups + g, 1), :]
            raw[KEY, to, cols] = (mixed * scale).astype(BF16)
        return 0

    lax.fori_loop(0, rows // tile, body, 0)


def per_device(
    n_sp,
    n_tp,
    tokens,
    input_norm_scale,
    mean_input_weight,
    query_matrix,
    key_matrix,
    value_matrix,
    strength_weight,
    decay_input_weight,
    causal_filter_weight,
    head_decay_logrates,
    decay_input_shift,
    strength_shift,
    decay_spike,
    head_norm_scale,
    group_mixing_weight,
    mean_channel_scale,
    mean_output_weight,
    delta_output_weight,
):
    rows, dim = tokens.shape
    rows_in, width = key_matrix.shape
    heads = strength_weight.shape[1]
    depth = width // heads
    rows_out, cols_out = mean_output_weight.shape
    n_y = n_tp // 2
    share = rows // n_tp
    groups = mean_input_weight.shape[1] // GROUP_DIM
    hops = n_sp // 2
    grid_x = 1
    while grid_x * grid_x * 4 <= n_sp:
        grid_x *= 2
    split = min(SPLIT, cols_out // 128)
    n_items = 2 * hops + 2 * (2 * (hops - 1) + 1) + split * (hops - 1) + split // 2
    any_ = pl.BlockSpec(memory_space=pl.ANY)
    vmem = pl.BlockSpec(memory_space=pltpu.VMEM)
    dma = pltpu.SemaphoreType.DMA
    return pl.pallas_call(
        lambda *refs: mixer_kernel((n_sp, n_tp, heads, depth, grid_x), *refs),
        out_shape=jax.ShapeDtypeStruct((share, dim), BF16),
        in_specs=[any_, vmem, any_, any_, any_, any_] + [vmem] * 8 + [any_, vmem, any_, any_],
        out_specs=any_,
        scratch_shapes=[
            pltpu.VMEM((4, n_sp, rows_in + PAD, width), BF16),
            pltpu.VMEM((split, n_sp, 2 * rows_out, cols_out // split), BF16),
            pltpu.VMEM((n_sp, rows + PAD, rows_in), BF16),
            pltpu.VMEM((4, rows + PAD, width), F32),
            pltpu.VMEM((4, rows + PAD, width), BF16),
            pltpu.VMEM((2, depth, dim), BF16),
            pltpu.VMEM((PAD, dim), BF16),
            pltpu.VMEM((rows, PAD), F32),
            pltpu.VMEM((rows // min(CHUNK, rows), heads, min(CHUNK, rows)), F32),
            pltpu.VMEM((PAD, width), BF16),
            pltpu.VMEM((1, dim), F32),
            pltpu.VMEM((mean_channel_scale.shape[0] // GROUP_DIM, GROUP_DIM), F32),
            pltpu.VMEM((groups, GROUP_DIM, GROUP_DIM), BF16),
            pltpu.VMEM((heads, depth, 2 * depth), F32),
            pltpu.VMEM((3, heads, depth, 2 * depth), BF16),
            pltpu.VMEM((3, heads, depth, 2 * depth), BF16),
            pltpu.VMEM((2, n_y, 2, share, cols_out // split), BF16),
            pltpu.VMEM((split * hops, n_y, 2, share, cols_out // split), BF16),
            pltpu.VMEM((split * hops, n_y - 1, 2, share, cols_out // split), BF16),
            pltpu.VMEM((split * hops, n_y - 1, 2, share, cols_out // split), BF16),
            pltpu.VMEM((2, 2, share, cols_out // split), BF16),
            dma((n_items, 2)),
            dma((n_items, 2)),
            dma((6 + 2 * split,)),
            dma((2,)),
            dma((2,)),
            dma((1 + grid_x,)),
            dma((3,)),
            dma((split * hops,)),
            dma((split * hops,)),
            dma((split * hops, n_y - 1)),
            dma((split * hops, n_y - 1)),
            dma((2, 2)),
        ],
        compiler_params=pltpu.CompilerParams(
            collective_id=0, has_side_effects=True, vmem_limit_bytes=64500000
        ),
    )(
        tokens,
        input_norm_scale.reshape(-1, 128),
        key_matrix,
        value_matrix,
        query_matrix,
        mean_input_weight,
        strength_weight.T,
        decay_input_weight.T,
        jnp.transpose(causal_filter_weight, (1, 0, 2)),
        head_decay_logrates.reshape(1, -1),
        decay_input_shift.reshape(1, -1),
        strength_shift.reshape(1, -1),
        decay_spike.T,
        head_norm_scale.reshape(1, -1),
        group_mixing_weight,
        mean_channel_scale.reshape(-1, GROUP_DIM),
        mean_output_weight,
        delta_output_weight,
    )


def solution(mesh):
    n_sp, n_tp = mesh.shape["sp"], mesh.shape["tp"]
    return jax.shard_map(
        lambda *args: per_device(n_sp, n_tp, *args),
        mesh=mesh,
        in_specs=(
            P("sp", None),
            P(),
            P("sp", "tp"),
            P("sp", "tp"),
            P("sp", "tp"),
            P("sp", "tp"),
            P("sp", "tp"),
            P("sp", "tp"),
            P(),
            P(),
            P(),
            P(),
            P("sp", "tp"),
            P(),
            P(),
            P(),
            P("tp", "sp"),
            P("tp", "sp"),
        ),
        out_specs=P(("sp", "tp"), None),
        check_vma=False,
    )
```

```python
import jax
import jax.numpy as jnp
from jax import lax
from jax.experimental import pallas as pl
from jax.experimental.pallas import tpu as pltpu
from jax.sharding import PartitionSpec as P

GROUP_DIM = 128
CONV = 4
EPSILON = 1e-06
PAD = 16
CHUNK = 128
BF16 = jnp.bfloat16
F32 = jnp.float32
MESH = pl.DeviceIdType.MESH
STATE_PART = 0.12
LAST_SINGLE = 2
MIDDLE = 2
SPLIT = 2
QUERY_PART = 0.03
KEY, VAL, QRY, POOL = range(4)


def dot(left, right):
    return jnp.dot(left.astype(BF16), right.astype(BF16), preferred_element_type=F32)


def dot_nt(left, right):
    return lax.dot_general(
        left.astype(BF16),
        right.astype(BF16),
        (((1,), (1,)), ((), ())),
        preferred_element_type=F32,
    )


def dot_tn(left, right):
    return lax.dot_general(
        left.astype(BF16),
        right.astype(BF16),
        (((0,), (0,)), ((), ())),
        preferred_element_type=F32,
    )


def unit_rows(values):
    return values * lax.rsqrt(jnp.sum(values * values, axis=-1, keepdims=True) + EPSILON)


def convolve(extended, taps, chunk):
    extended = extended.astype(F32)
    total = jnp.zeros((chunk, extended.shape[1]), F32)
    for i in range(CONV):
        start = PAD - (CONV - 1) + i
        total = total + taps[i] * extended[start : start + chunk]
    return total / (1.0 + jnp.exp(-total))


def decay_weights(cum_cols, cum_rows, h, causal):
    spread = cum_cols[:, h : h + 1] - cum_rows[h : h + 1, :]
    return jnp.where(causal, jnp.exp(jnp.where(causal, spread, 0.0)), 0.0)


def state_chunk(heads, depth, chunk, convolved, beta, decay, carry):
    row = lax.broadcasted_iota(jnp.int32, (chunk, chunk), 0)
    col = lax.broadcasted_iota(jnp.int32, (chunk, chunk), 1)
    causal = row >= col
    strict = row > col
    eye = jnp.where(row == col, 1.0, 0.0)
    tri = jnp.where(causal, 1.0, 0.0)
    cum_cols = jnp.dot(tri, decay, preferred_element_type=F32, precision=lax.Precision.HIGHEST)
    cum_rows = lax.dot_general(
        decay,
        tri,
        (((0,), (1,)), ((), ())),
        preferred_element_type=F32,
        precision=lax.Precision.HIGHEST,
    )
    base = min(16, chunk)
    hs = range(heads)
    k = [unit_rows(convolved[0][:, h * depth : (h + 1) * depth]) for h in hs]
    v = [convolved[1][:, h * depth : (h + 1) * depth] for h in hs]
    cum = [cum_cols[:, h : h + 1] for h in hs]
    last = [cum_cols[chunk - 1 : chunk, h : h + 1] for h in hs]
    beta = [beta[:, h : h + 1] for h in hs]
    weights = [decay_weights(cum_cols, cum_rows, h, causal) for h in hs]
    kb = [k[h] * beta[h] for h in hs]
    lower = [jnp.where(strict, dot_nt(kb[h], k[h]) * weights[h], 0.0) for h in hs]
    power = [jnp.where(row // base == col // base, lower[h], 0.0) for h in hs]
    inverse = [eye - power[h] for h in hs]
    reach = 2
    while reach < base:
        power = [dot(power[h], power[h]) for h in hs]
        inverse = [inverse[h] + dot(inverse[h], power[h]) for h in hs]
        reach *= 2
    size = base
    while size < chunk:
        pair = (row // (2 * size) == col // (2 * size)) & (row // size != col // size)
        right = [dot(jnp.where(pair, lower[h], 0.0), inverse[h]) for h in hs]
        inverse = [inverse[h] - dot(inverse[h], right[h]) for h in hs]
        size *= 2
    grow = [jnp.exp(cum[h]) for h in hs]
    sides = [jnp.concatenate([v[h] * beta[h], kb[h] * grow[h]], axis=1) for h in hs]
    solved = [dot(inverse[h], sides[h]) for h in hs]
    kd = [k[h] * jnp.exp(last[h] - cum[h]) for h in hs]
    zeros = jnp.zeros((chunk, depth), F32)
    state = [carry[h] for h in hs]
    fresh = [
        jnp.concatenate([solved[h][:, :depth], zeros], axis=1) - dot(solved[h][:, depth:], state[h])
        for h in hs
    ]
    for h in hs:
        carry[h] = state[h] * jnp.exp(last[h]) + dot_tn(kd[h], fresh[h])
    return k, cum_cols, cum_rows, state, fresh


class Ring:
    def __init__(self, hops, split, subs, half_rows, refs, sems, owner, peers, window):
        self.refs, self.sems, self.owner, self.peers, self.window = refs, sems, owner, peers, window
        self.items = []
        self.index = {}
        rows_in, rows_out = half_rows
        top = rows_in // 2
        for j in range(1, hops + 1):
            for m in (KEY, VAL):
                full = rows_in + PAD if m == KEY else rows_in
                if j < hops:
                    self.add(("in", m, 0), j, [("in", m, 0, full)] * 2)
                else:
                    self.add(("in", m, 0), j, [("in", m, 0, top), ("in", m, top, full)])
        for j in range(1, hops + 1):
            for m in (QRY, POOL):
                if j < hops:
                    self.add(("in", m, 0), j, [("in", m, 0, top)] * 2)
                    self.add(("in", m, 1), j, [("in", m, top, rows_in)] * 2)
                else:
                    self.add(("in", m, 0), j, [("in", m, 0, top), ("in", m, top, rows_in)])
        for j in range(1, hops + 1):
            if j < hops:
                for e in range(split):
                    self.add(("out", e, 0), j, [("out", e, 0, rows_out)] * 2)
            else:
                for e in range(split // 2):
                    for c in range(subs):
                        ends = [("out", e, 0, rows_out, c), ("out", split // 2 + e, 0, rows_out, c)]
                        self.add(("out", e, c), j, ends)
        self.finish = []
        total = 0
        for _, _, parts in self.items:
            total += (parts[0][3] - parts[0][2]) * refs[parts[0][0]].shape[3] // (
                subs if len(parts[0]) == 5 else 1
            )
            self.finish.append(total)
        self.total = total
        self.subs = subs
        self.started = 0
        self.sent = set()
        self.received = set()

    def add(self, key, j, parts):
        self.index[key + (j,)] = len(self.items)
        self.items.append((key, j, parts))

    def copy(self, i, side):
        key, j, parts = self.items[i]
        kind, m, low, high = parts[side][:4]
        ref = self.refs[kind]
        wide = ref.shape[3] // (self.subs if len(parts[side]) == 5 else 1)
        cols = pl.ds(parts[side][4] * wide if len(parts[side]) == 5 else 0, wide)
        block = ref.at[m, self.owner(-(j - 1) if side == 0 else j - 1), pl.ds(low, high - low), cols]
        return pltpu.make_async_remote_copy(
            src_ref=block,
            dst_ref=block,
            send_sem=self.sems[0].at[i, side],
            recv_sem=self.sems[1].at[i, side],
            device_id=self.peers[side],
            device_id_type=MESH,
        )

    def arrive(self, i, side):
        if (i, side) in self.received:
            return
        self.received.add((i, side))
        self.copy(i, side).wait_recv()

    def leave(self, i):
        if i in self.sent:
            return
        self.sent.add(i)
        for side in range(2):
            self.copy(i, side).wait_send()

    def start_next(self):
        i = self.started
        if i >= len(self.items):
            return
        behind = i - self.ahead(i)
        if behind >= 0:
            self.leave(behind)
        key, j, parts = self.items[i]
        for side in range(2):
            if j > 1:
                kind, m, low, high = parts[side][:4]
                for before in range(i):
                    other, hop, pieces = self.items[before]
                    if hop == j - 1 and pieces[side][:2] == (kind, m) and pieces[side][2] <= low < pieces[side][3]:
                        self.arrive(before, side)
                    elif hop == j - 1 and pieces[side][:2] == (kind, m) and low <= pieces[side][2] < high:
                        self.arrive(before, side)
            self.copy(i, side).start()
        self.started += 1

    def ahead(self, i):
        if i >= len(self.items) - LAST_SINGLE:
            return 1
        return MIDDLE if self.items[i][0][1] in (QRY, POOL) and self.items[i][0][0] == "in" else 2

    def tick(self, part):
        while self.started < len(self.items):
            behind = self.started - self.ahead(self.started)
            if behind >= 0 and self.finish[behind] > part * self.total:
                break
            self.start_next()

    def need(self, key):
        i = self.index[key]
        while self.started < len(self.items) and self.started - self.ahead(self.started) <= i:
            self.start_next()
        for side in range(2):
            self.arrive(i, side)

    def close(self):
        while self.started < len(self.items):
            self.start_next()
        for i in range(len(self.items)):
            for side in range(2):
                self.arrive(i, side)
            self.leave(i)


def mixer_kernel(cfg, *refs):
    (
        tok_ref, gain_ref, wk_ref, wv_ref, wq_ref, wp_ref, strength_ref, slow_ref, tap_ref, rate_ref,
        dshift_ref, sshift_ref, spike_ref, hgain_ref, gmw_ref, cscale_ref, wpo_ref, wdo_ref,
    ) = refs[:18]
    out_ref = refs[18]
    (
        win, wout, normed, acc, raw, stage, before_tok, nraw, rowcum, tail, gain, cscale, gmw, carry, held,
        caught, psend, corerecv, ysend, yrecv, obuf, ring_send, ring_recv, local_sem, tok_sem, halo_sem,
        scan_send, scan_recv, core_send, core_recv, y_send, y_recv, out_sem,
    ) = refs[19:]
    n_sp, n_tp, heads, depth, grid_x, subs = cfg
    grid_z = n_sp // grid_x
    hops = n_sp // 2
    n_y = n_tp // 2
    rows, width = raw.shape[1] - PAD, raw.shape[2]
    rows_in = normed.shape[2]
    split, rows_out, cols_half = wout.shape[0], wout.shape[2] // 2, wout.shape[3]
    share = rows // n_tp
    sp = lax.axis_index("sp")
    tp = lax.axis_index("tp")
    core = tp % 2
    ypos = tp // 2

    def sp_at(r):
        s = jnp.maximum(r - grid_z, 0)
        i = s // (grid_x - 1)
        k = s % (grid_x - 1)
        x = 1 + jnp.where(i % 2 == 0, k, grid_x - 2 - k)
        return jnp.where(r < grid_z, r * grid_x, (grid_z - 1 - i) * grid_x + x)

    zc = sp // grid_x
    xc = sp % grid_x
    ic = grid_z - 1 - zc
    kc = jnp.where(ic % 2 == 0, xc - 1, grid_x - 1 - xc)
    pos = jnp.where(xc == 0, zc, grid_z + ic * (grid_x - 1) + kc)

    def owner(offset):
        return sp_at((pos + offset + n_sp) % n_sp)

    barrier = pltpu.get_barrier_semaphore()
    for k in range(1, n_sp):
        pl.semaphore_signal(barrier, inc=1, device_id=((sp + k) % n_sp, tp), device_id_type=MESH)
    for k in range(1, n_tp):
        pl.semaphore_signal(barrier, inc=1, device_id=(sp, (tp + k) % n_tp), device_id_type=MESH)

    locals_ = []

    def bring(src, dst):
        locals_.append(pltpu.make_async_copy(src, dst, local_sem.at[len(locals_)]))
        locals_[-1].start()

    groups = gmw.shape[0]
    bring(wk_ref, win.at[KEY, sp, pl.ds(0, rows_in), :])
    bring(wv_ref, win.at[VAL, sp, pl.ds(0, rows_in), :])
    bring(wq_ref, win.at[QRY, sp, pl.ds(0, rows_in), :])
    bring(wp_ref, win.at[POOL, sp, pl.ds(0, rows_in), :])
    for half in range(split):
        cols = pl.ds(half * cols_half, cols_half)
        bring(wpo_ref.at[:, cols], wout.at[half, sp, pl.ds(0, rows_out), :])
        bring(wdo_ref.at[:, cols], wout.at[half, sp, pl.ds(rows_out, rows_out), :])
    bring(gmw_ref.at[pl.ds(tp * groups, groups)], gmw)
    step_rows = stage.shape[1]
    n_stage = rows // step_rows

    def token_copy(t, slot):
        return pltpu.make_async_copy(
            tok_ref.at[pl.ds(pl.multiple_of(t * step_rows, step_rows), step_rows), :],
            stage.at[slot],
            tok_sem.at[slot],
        )

    token_copy(0, 0).start()
    win[KEY, sp, pl.ds(rows_in, PAD), pl.ds(0, rows_in)] = jnp.concatenate(
        [
            strength_ref[...].astype(F32),
            slow_ref[...].astype(F32),
            jnp.zeros((PAD - 2 * heads, rows_in), F32),
        ],
        axis=0,
    ).astype(BF16)
    for i in range(gain_ref.shape[0]):
        gain[:, i * 128 : (i + 1) * 128] = gain_ref[i : i + 1, :].astype(F32)
    cscale[...] = cscale_ref[...].astype(F32)
    locals_[0].wait()
    locals_[1].wait()
    pl.semaphore_wait(barrier, n_sp + n_tp - 2)

    part = tok_ref.shape[1] // n_tp
    my_part = pl.ds(pl.multiple_of(tp * part, 128), part)
    halo = pltpu.make_async_remote_copy(
        src_ref=tok_ref.at[pl.ds(rows - PAD, PAD), my_part],
        dst_ref=before_tok.at[:, my_part],
        send_sem=halo_sem.at[0, 0],
        recv_sem=halo_sem.at[1, 0],
        device_id=((sp + 1) % n_sp, tp),
        device_id_type=MESH,
    )
    spread = [
        pltpu.make_async_remote_copy(
            src_ref=before_tok.at[:, my_part],
            dst_ref=before_tok.at[:, my_part],
            send_sem=halo_sem.at[0, k],
            recv_sem=halo_sem.at[1, k],
            device_id=(sp, (tp + k) % n_tp),
            device_id_type=MESH,
        )
        for k in range(1, n_tp)
    ]

    @pl.when(sp + 1 < n_sp)
    def _():
        halo.start()

    ring = Ring(
        hops,
        split,
        subs,
        (rows_in, wout.shape[2]),
        {"in": win, "out": wout},
        (ring_send, ring_recv),
        owner,
        [(owner(1), tp), (owner(-1), tp)],
        2,
    )
    ring.tick(0.0)
    for c in locals_[2:]:
        c.wait()

    @pl.when(sp > 0)
    def _():
        halo.wait_recv()
        for c in spread:
            c.start()

    def norm_rows(load, to, count):
        squares = jnp.zeros((count, 1), F32)
        for b in range(n_sp):
            x = load(slice(b * rows_in, (b + 1) * rows_in)).astype(F32)
            squares = squares + jnp.sum(x * x, axis=-1, keepdims=True)
        scale = lax.rsqrt(squares * (1.0 / (n_sp * rows_in)) + EPSILON)
        for b in range(n_sp):
            cols = slice(b * rows_in, (b + 1) * rows_in)
            normed[b, to, :] = (load(cols).astype(F32) * scale * gain[:, cols]).astype(BF16)

    def norm_step(t, _):
        slot = t % 2
        token_copy(t, slot).wait()

        @pl.when(t + 1 < n_stage)
        def _():
            token_copy(t + 1, 1 - slot).start()

        def piece(u, _):
            at = pl.ds(pl.multiple_of(u * 32, 32), 32)
            to = pl.ds(pl.multiple_of(PAD + t * step_rows + u * 32, PAD), 32)
            norm_rows(lambda cols: stage[slot, at, cols], to, 32)
            return 0

        lax.fori_loop(0, step_rows // 32, piece, 0)
        return 0

    lax.fori_loop(0, n_stage, norm_step, 0)

    @pl.when(sp > 0)
    def _():
        for c in spread:
            c.wait_recv()

    @pl.when(sp == 0)
    def _():
        before_tok[...] = jnp.zeros(before_tok.shape, BF16)

    norm_rows(lambda cols: before_tok[:, cols], pl.ds(0, PAD), PAD)

    tile = max(d for d in range(PAD, 273, PAD) if (rows + PAD) % d == 0)
    n_tile = (rows + PAD) // tile

    def project(m, owners, first=False, final=False):
        def body(t, _):
            at = pl.ds(pl.multiple_of(t * tile, PAD), tile)
            total = None if first else acc[m, at, :]
            for o in owners:
                term = jnp.dot(
                    normed[o, at, :], win[m, o, pl.ds(0, rows_in), :], preferred_element_type=F32
                )
                total = term if total is None else total + term
            if final:
                raw[m, at, :] = total.astype(BF16)
            else:
                acc[m, at, :] = total
            return 0

        lax.fori_loop(0, n_tile, body, 0)

    def own(m, _):
        project(m, [sp], first=True)
        return 0

    lax.fori_loop(0, 4, own, 0)

    def arriving(i, _):
        for k in range(2 * hops):
            @pl.when(i == k)
            def _():
                ring.need(("in", k % 2, 0, k // 2 + 1))

        m, j = i % 2, i // 2 + 1

        @pl.when(j < hops)
        def _():
            project(m, [owner(-j), owner(j)])

        @pl.when(j == hops)
        def _():
            project(m, [owner(hops)], final=True)

        return 0

    lax.fori_loop(0, 2 * hops, arriving, 0)
    block = min(256, rows)
    n_block = rows // block

    def narrow_body(t, _):
        at = pl.ds(pl.multiple_of(t * block, block), block)
        total = jnp.zeros((block, PAD), F32)
        for o in range(n_sp):
            total = total + dot_nt(
                normed[o, pl.ds(pl.multiple_of(PAD + t * block, PAD), block), :],
                win[KEY, o, pl.ds(rows_in, PAD), pl.ds(0, rows_in)],
            )
        nraw[at, :] = total
        return 0

    lax.fori_loop(0, n_block, narrow_body, 0)

    lane = lax.broadcasted_iota(jnp.int32, (1, rate_ref.shape[1]), 1)
    small = lax.broadcasted_iota(jnp.int32, (1, heads), 1)

    def head_row(ref):
        total = jnp.zeros((1, heads), F32)
        for h in range(heads):
            value = jnp.sum(jnp.where(lane == tp * heads + h, ref[...], 0.0), axis=-1, keepdims=True)
            total = total + jnp.where(small == h, value, 0.0)
        return total

    speed = -jnp.exp(head_row(rate_ref))
    dshift = head_row(dshift_ref)
    sshift = head_row(sshift_ref)
    mine = pl.ds(pl.multiple_of(tp * width, 128), width)
    wide = lax.broadcasted_iota(jnp.int32, (depth, 2 * depth), 1)
    sub = lax.broadcasted_iota(jnp.int32, (depth, 2 * depth), 0)
    for h in range(heads):
        carry[h] = jnp.where(wide == sub + depth, 1.0, 0.0)
    chunk = min(CHUNK, rows)
    n_chunk = rows // chunk
    tail[...] = raw[KEY, pl.ds(0, PAD), :]
    one = lax.broadcasted_iota(jnp.int32, (heads, heads), 0) == lax.broadcasted_iota(
        jnp.int32, (heads, heads), 1
    )
    per_slot = stage.shape[2] // (2 * depth)
    fresh_at = [((h * 2 * depth) // width, (h * 2 * depth) % width) for h in range(heads)]

    def stage_at(c, h):
        flat = c * heads + h
        cols = pl.ds(pl.multiple_of((flat % per_slot) * 2 * depth, 128), 2 * depth)
        return stage.at[flat // per_slot, pl.ds(0, depth), cols]

    third = 1.0 / 3.0

    def state_step(c, _):
        for k in range(n_chunk):
            @pl.when(c == k)
            def _():
                ring.tick(third + STATE_PART * k / n_chunk)

        at = pl.ds(pl.multiple_of(c * chunk, chunk), chunk)
        to = pl.ds(pl.multiple_of(PAD + c * chunk, PAD), chunk)
        window = pl.ds(pl.multiple_of(c * chunk, chunk), chunk + PAD)
        keys = jnp.concatenate([tail[...], raw[KEY, to, :]], axis=0)
        tail[...] = keys[chunk:]
        taps = [[tap_ref[r, i : i + 1, mine].astype(F32) for i in range(CONV)] for r in range(3)]
        convolved = [convolve(keys, taps[1], chunk), convolve(raw[VAL, window, :], taps[2], chunk)]
        narrow = nraw[at, :].astype(BF16).astype(F32)
        beta = 1.0 / (1.0 + jnp.exp(-(narrow[:, :heads] + sshift)))
        x = narrow[:, heads : 2 * heads] + dshift
        soft = jnp.maximum(x, 0.0) + jnp.log1p(jnp.exp(-jnp.abs(x)))
        spike = lax.dot_general(
            spike_ref[:, at],
            jnp.where(one, 1.0, 0.0),
            (((0,), (0,)), ((), ())),
            preferred_element_type=F32,
            precision=lax.Precision.HIGHEST,
        )
        decay = speed * soft + spike
        k, cum_cols, cum_rows, state, fresh = state_chunk(
            heads, depth, chunk, convolved, beta, decay, carry
        )
        nraw[at, pl.ds(0, heads)] = cum_cols
        rowcum[c] = cum_rows
        for h in range(heads):
            raw[KEY, to, h * depth : (h + 1) * depth] = k[h].astype(BF16)
            stage_at(c, h)[...] = state[h].astype(BF16)
            slot, low = fresh_at[h]
            acc[slot, at, low : low + 2 * depth] = fresh[h]
        return 0

    lax.fori_loop(0, n_chunk, state_step, 0)

    far = grid_x - 1
    whole, front = pl.ds(0, 2 * depth), pl.ds(0, depth)

    def pass_state(slot, source, target, pick, z, x):
        return pltpu.make_async_remote_copy(
            src_ref=source.at[:, :, pick],
            dst_ref=caught.at[target, :, :, pick],
            send_sem=scan_send.at[slot],
            recv_sem=scan_recv.at[target],
            device_id=(z * grid_x + x, tp),
            device_id_type=MESH,
        )

    along_x = pass_state(0, held.at[0], 0, whole, zc, (xc + 1) % grid_x)
    along_z = pass_state(1, held.at[1], 1, front, (zc + 1) % grid_z, xc)
    back = [
        pass_state(2 + x, caught.at[1], 2, front, zc, (xc + 1 + x) % grid_x) for x in range(far)
    ]

    @pl.when(xc == 0)
    def _():
        for h in range(heads):
            held[0, h] = carry[h].astype(BF16)
            caught[0, h] = jnp.where(wide == sub + depth, 1.0, 0.0).astype(BF16)
        along_x.start()

    def x_stage(x):
        @pl.when(xc == x)
        def _():
            along_x.wait_recv()
            for h in range(heads):
                later = carry[h]
                pushed = dot(later[:, depth:], caught[0, h])
                held[0, h, :, front] = (later[:, :depth] + pushed[:, :depth]).astype(BF16)
                held[0, h, :, pl.ds(depth, depth)] = pushed[:, depth:].astype(BF16)
            if x < far:
                along_x.start()

    def z_stage(z):
        @pl.when((xc == far) & (zc == z))
        def _():
            if z == 0:
                for h in range(heads):
                    caught[1, h, :, front] = jnp.zeros((depth, depth), BF16)
            else:
                along_z.wait_recv()
                for c in back:
                    c.start()
            if z + 1 < grid_z:
                for h in range(heads):
                    later = held[0, h]
                    pushed = dot(later[:, depth:], caught[1, h, :, front])
                    held[1, h, :, front] = (later[:, :depth].astype(F32) + pushed).astype(BF16)
                along_z.start()

    def last_stage():
        @pl.when((xc < far) & (zc > 0))
        def _():
            back[0].wait_recv()
            for h in range(heads):
                caught[1, h, :, front] = caught[2, h, :, front]

        @pl.when((xc < far) & (zc == 0))
        def _():
            for h in range(heads):
                caught[1, h, :, front] = jnp.zeros((depth, depth), BF16)

        for h in range(heads):
            later = caught[0, h]
            pushed = dot(later[:, depth:], caught[1, h, :, front])
            held[2, h, :, front] = (later[:, :depth].astype(F32) + pushed).astype(BF16)

    incoming = held.at[2]

    def hop(m, j):
        ring.need(("in", m, 0, j))
        if j < hops:
            ring.need(("in", m, 1, j))
            project(m, [owner(-j), owner(j)])
        else:
            project(m, [owner(hops)], final=True)

    steps = [(m, j) for j in range(1, hops + 1) for m in (QRY, POOL)][:-1]
    for i, (m, j) in enumerate(steps):
        hop(m, j)
        if 2 <= i <= far + 1:
            x_stage(i - 1)
        if far < i <= far + grid_z:
            z_stage(i - far - 1)
    last_stage()

    hgain = hgain_ref[...].astype(F32)
    row = lax.broadcasted_iota(jnp.int32, (chunk, chunk), 0)
    col = lax.broadcasted_iota(jnp.int32, (chunk, chunk), 1)
    causal = row >= col

    def query_step(c, _):
        for k in range(n_chunk):
            @pl.when(c == k)
            def _():
                ring.tick(2 * third - 0.02 + QUERY_PART * k / n_chunk)

        at = pl.ds(pl.multiple_of(c * chunk, chunk), chunk)
        to = pl.ds(pl.multiple_of(PAD + c * chunk, PAD), chunk)
        window = pl.ds(pl.multiple_of(c * chunk, chunk), chunk + PAD)
        taps = [tap_ref[0, i : i + 1, mine].astype(F32) for i in range(CONV)]
        convolved = convolve(raw[QRY, window, :], taps, chunk)
        cum_cols = nraw[at, :]
        cum_rows = rowcum[c]
        hs = range(heads)
        spans = [slice(h * depth, (h + 1) * depth) for h in hs]
        q = [unit_rows(convolved[:, spans[h]]) * depth ** (-0.5) for h in hs]
        weights = [decay_weights(cum_cols, cum_rows, h, causal) for h in hs]
        scores = [dot_nt(q[h], raw[KEY, to, spans[h]]) * weights[h] for h in hs]
        grow = [jnp.exp(cum_cols[:, h : h + 1]) for h in hs]
        outs = []
        for h in hs:
            slot, low = fresh_at[h]
            outs.append(
                dot(q[h] * grow[h], stage_at(c, h)[...])
                + dot(scores[h], acc[slot, at, low : low + 2 * depth])
            )
        values = [
            outs[h][:, :depth] + dot(outs[h][:, depth:], incoming[h, :, pl.ds(0, depth)]) for h in hs
        ]
        for h in hs:
            scale = lax.rsqrt(jnp.mean(values[h] * values[h], axis=-1, keepdims=True) + EPSILON)
            raw[VAL, to, spans[h]] = (values[h] * scale * hgain).astype(BF16)
        return 0

    lax.fori_loop(0, n_chunk, query_step, 0)
    hop(POOL, hops)
    pool_mix(cfg, raw, gmw, cscale, sp, tp, block, rows, width)

    n_pair = split * hops

    def half_of(p, u):
        q = jnp.maximum(p - split // 2, 0)
        t = p - (n_pair - split // 2)
        step = jnp.where(p < split // 2, 0, q // split + 1)
        part = jnp.where(
            p < split // 2, 2 * p + u, jnp.where(t >= 0, u * (split // 2) + t, q % split)
        )
        return owner((2 * u - 1) * step), part

    n_turn = n_pair - 1 + subs

    def turn(b):
        if isinstance(b, int) and b >= n_pair - 1 and subs > 1:
            return n_pair - 1, (b - n_pair + 1) * (cols_half // subs), cols_half // subs
        return b, 0, cols_half

    def partial(dest, b, u):
        p, low, wide_b = turn(b)
        o, half = half_of(p, u)
        at = pl.ds(pl.multiple_of(PAD + dest * share, PAD), share)
        cols = pl.ds(low, wide_b)
        total = jnp.dot(
            raw[KEY, at, :], wout[half, o, pl.ds(0, rows_out), cols], preferred_element_type=F32
        ) + jnp.dot(
            raw[VAL, at, :], wout[half, o, pl.ds(rows_out, rows_out), cols], preferred_element_type=F32
        )
        return total.astype(BF16)

    def core_copy(b):
        cols = pl.ds(0, turn(b)[2])
        return pltpu.make_async_remote_copy(
            src_ref=psend.at[b % 2, :, :, :, cols],
            dst_ref=corerecv.at[b, :, :, :, cols],
            send_sem=core_send.at[b],
            recv_sem=core_recv.at[b],
            device_id=(sp, ypos * 2 + 1 - core),
            device_id_type=MESH,
        )

    def y_copy(b, d):
        cols = pl.ds(0, turn(b)[2])
        return pltpu.make_async_remote_copy(
            src_ref=ysend.at[b, d - 1, :, :, cols],
            dst_ref=yrecv.at[b, d - 1, :, :, cols],
            send_sem=y_send.at[b, d - 1],
            recv_sem=y_recv.at[b, d - 1],
            device_id=(sp, ((ypos + d) % n_y) * 2 + core),
            device_id_type=MESH,
        )

    def out_copy(b, u):
        p, low, wide_b = turn(b)
        o, half = half_of(p, u)
        start = pl.multiple_of((o * split + half) * cols_half + low, 128)
        return pltpu.make_async_copy(
            obuf.at[b % 2, u, :, pl.ds(0, wide_b)],
            out_ref.at[:, pl.ds(start, wide_b)],
            out_sem.at[b % 2, u],
        )

    def own_at(b, u):
        at = pl.ds(pl.multiple_of((b % 4) * share, share), share)
        return acc.at[QRY, at, pl.ds(u * cols_half, turn(b)[2])]

    def stage_one(b):
        @pl.when(b >= 2)
        def _():
            core_copy(b - 2).wait_send()

        cols = pl.ds(0, turn(b)[2])
        for u in range(2):
            for y in range(n_y):
                psend[b % 2, y, u, :, cols] = partial(y * 2 + 1 - core, b, u)
        core_copy(b).start()

    def stage_two(b):
        cols = pl.ds(0, turn(b)[2])
        parts = [
            [partial(((ypos + d) % n_y) * 2 + core, b, u) for d in range(n_y)] for u in range(2)
        ]
        core_copy(b).wait_recv()
        for d in range(1, n_y):
            there = (ypos + d) % n_y
            for u in range(2):
                total = parts[u][d].astype(F32) + corerecv[b, there, u, :, cols].astype(F32)
                ysend[b, d - 1, u, :, cols] = total.astype(BF16)
            y_copy(b, d).start()
        for u in range(2):
            own_at(b, u)[...] = parts[u][0].astype(F32) + corerecv[b, ypos, u, :, cols].astype(F32)

    def stage_three(b):
        cols = pl.ds(0, turn(b)[2])
        for d in range(1, n_y):
            y_copy(b, d).wait_recv()
        for u in range(2):
            total = own_at(b, u)[...]
            for d in range(1, n_y):
                total = total + yrecv[b, d - 1, u, :, cols].astype(F32)

            @pl.when(b >= 2)
            def _():
                out_copy(b - 2, u).wait()

            obuf[b % 2, u, :, cols] = total.astype(BF16)
            out_copy(b, u).start()

    def out_step(p, _):
        for i in range(n_pair - 1):
            @pl.when(p == i)
            def _():
                if i < split // 2:
                    ring.tick(2 * third)
                else:
                    e = i - split // 2
                    ring.need(("out", e % split, 0, e // split + 1))

        stage_one(p)

        @pl.when(p >= 2)
        def _():
            stage_three(p - 2)

        stage_two(p)
        return 0

    lax.fori_loop(0, n_pair - 1, out_step, 0)
    for c in range(subs):
        ring.need(("out", split // 2 - 1, c, hops))
        stage_one(n_pair - 1 + c)
        if c == 0:
            stage_three(n_pair - 3)
        stage_two(n_pair - 1 + c)
    for b in range(n_pair - 2, n_turn):
        stage_three(b)
    ring.close()
    for b in range(n_turn - 2, n_turn):
        core_copy(b).wait_send()
        for u in range(2):
            out_copy(b, u).wait()

    def drain(b, _):
        for d in range(1, n_y):
            y_copy(b, d).wait_send()
        return 0

    lax.fori_loop(0, n_pair - 1, drain, 0)
    for b in range(n_pair - 1, n_turn):
        drain(b, 0)

    @pl.when(sp + 1 < n_sp)
    def _():
        halo.wait_send()

    @pl.when(sp > 0)
    def _():
        for c in spread:
            c.wait_send()

    @pl.when(xc < far)
    def _():
        along_x.wait_send()

    @pl.when((xc == far) & (zc + 1 < grid_z))
    def _():
        along_z.wait_send()

    @pl.when((xc == far) & (zc > 0))
    def _():
        for c in back:
            c.wait_send()


def pool_mix(cfg, raw, gmw, cscale, sp, tp, tile, rows, width):
    groups = gmw.shape[0]

    def body(t, _):
        window = pl.ds(pl.multiple_of(t * tile, tile), tile + PAD)
        to = pl.ds(pl.multiple_of(PAD + t * tile, PAD), tile)
        place = sp * rows + t * tile + lax.broadcasted_iota(jnp.int32, (tile, 1), 0) + 1
        for g in range(groups):
            cols = slice(g * GROUP_DIM, (g + 1) * GROUP_DIM)
            extended = raw[POOL, window, cols].astype(F32)
            sums = extended
            options = []
            for lag in (1, 2, 4, 8):
                sums = sums + pltpu.roll(sums, lag, 0)
                options.append(sums[PAD:])
            if groups % 4 == 0:
                size = 2 << (g % 4)
                windowed = options[g % 4]
            else:
                which = (tp * groups + g) % 4
                size = jnp.where(which == 0, 2, jnp.where(which == 1, 4, jnp.where(which == 2, 8, 16)))
                windowed = options[3]
                for i in range(3):
                    windowed = jnp.where(which == i, options[i], windowed)
            counts = jnp.minimum(place, size).astype(F32)
            diff = (windowed / counts - extended[PAD:]).astype(BF16)
            mixed = jnp.dot(diff, gmw[g], preferred_element_type=F32)
            scale = cscale[pl.ds(tp * groups + g, 1), :]
            raw[KEY, to, cols] = (mixed * scale).astype(BF16)
        return 0

    lax.fori_loop(0, rows // tile, body, 0)


def per_device(
    n_sp,
    n_tp,
    tokens,
    input_norm_scale,
    mean_input_weight,
    query_matrix,
    key_matrix,
    value_matrix,
    strength_weight,
    decay_input_weight,
    causal_filter_weight,
    head_decay_logrates,
    decay_input_shift,
    strength_shift,
    decay_spike,
    head_norm_scale,
    group_mixing_weight,
    mean_channel_scale,
    mean_output_weight,
    delta_output_weight,
):
    rows, dim = tokens.shape
    rows_in, width = key_matrix.shape
    heads = strength_weight.shape[1]
    depth = width // heads
    rows_out, cols_out = mean_output_weight.shape
    n_y = n_tp // 2
    share = rows // n_tp
    groups = mean_input_weight.shape[1] // GROUP_DIM
    hops = n_sp // 2
    grid_x = 1
    while grid_x * grid_x * 4 <= n_sp:
        grid_x *= 2
    split = min(SPLIT, cols_out // 128)
    subs = 2 if split == 2 and cols_out // split % 256 == 0 else 1
    n_items = 2 * hops + 2 * (2 * (hops - 1) + 1) + split * (hops - 1) + split // 2 * subs
    n_turn = split * hops - 1 + subs
    any_ = pl.BlockSpec(memory_space=pl.ANY)
    vmem = pl.BlockSpec(memory_space=pltpu.VMEM)
    dma = pltpu.SemaphoreType.DMA
    return pl.pallas_call(
        lambda *refs: mixer_kernel((n_sp, n_tp, heads, depth, grid_x, subs), *refs),
        out_shape=jax.ShapeDtypeStruct((share, dim), BF16),
        in_specs=[any_, vmem, any_, any_, any_, any_] + [vmem] * 8 + [any_, vmem, any_, any_],
        out_specs=any_,
        scratch_shapes=[
            pltpu.VMEM((4, n_sp, rows_in + PAD, width), BF16),
            pltpu.VMEM((split, n_sp, 2 * rows_out, cols_out // split), BF16),
            pltpu.VMEM((n_sp, rows + PAD, rows_in), BF16),
            pltpu.VMEM((4, rows + PAD, width), F32),
            pltpu.VMEM((4, rows + PAD, width), BF16),
            pltpu.VMEM((2, depth, dim), BF16),
            pltpu.VMEM((PAD, dim), BF16),
            pltpu.VMEM((rows, PAD), F32),
            pltpu.VMEM((rows // min(CHUNK, rows), heads, min(CHUNK, rows)), F32),
            pltpu.VMEM((PAD, width), BF16),
            pltpu.VMEM((1, dim), F32),
            pltpu.VMEM((mean_channel_scale.shape[0] // GROUP_DIM, GROUP_DIM), F32),
            pltpu.VMEM((groups, GROUP_DIM, GROUP_DIM), BF16),
            pltpu.VMEM((heads, depth, 2 * depth), F32),
            pltpu.VMEM((3, heads, depth, 2 * depth), BF16),
            pltpu.VMEM((3, heads, depth, 2 * depth), BF16),
            pltpu.VMEM((2, n_y, 2, share, cols_out // split), BF16),
            pltpu.VMEM((n_turn, n_y, 2, share, cols_out // split), BF16),
            pltpu.VMEM((n_turn, n_y - 1, 2, share, cols_out // split), BF16),
            pltpu.VMEM((n_turn, n_y - 1, 2, share, cols_out // split), BF16),
            pltpu.VMEM((2, 2, share, cols_out // split), BF16),
            dma((n_items, 2)),
            dma((n_items, 2)),
            dma((6 + 2 * split,)),
            dma((2,)),
            dma((2, n_tp)),
            dma((1 + grid_x,)),
            dma((3,)),
            dma((n_turn,)),
            dma((n_turn,)),
            dma((n_turn, n_y - 1)),
            dma((n_turn, n_y - 1)),
            dma((2, 2)),
        ],
        compiler_params=pltpu.CompilerParams(
            collective_id=0, has_side_effects=True, vmem_limit_bytes=67043328
        ),
    )(
        tokens,
        input_norm_scale.reshape(-1, 128),
        key_matrix,
        value_matrix,
        query_matrix,
        mean_input_weight,
        strength_weight.T,
        decay_input_weight.T,
        jnp.transpose(causal_filter_weight, (1, 0, 2)),
        head_decay_logrates.reshape(1, -1),
        decay_input_shift.reshape(1, -1),
        strength_shift.reshape(1, -1),
        decay_spike.T,
        head_norm_scale.reshape(1, -1),
        group_mixing_weight,
        mean_channel_scale.reshape(-1, GROUP_DIM),
        mean_output_weight,
        delta_output_weight,
    )


def solution(mesh):
    n_sp, n_tp = mesh.shape["sp"], mesh.shape["tp"]
    return jax.shard_map(
        lambda *args: per_device(n_sp, n_tp, *args),
        mesh=mesh,
        in_specs=(
            P("sp", None),
            P(),
            P("sp", "tp"),
            P("sp", "tp"),
            P("sp", "tp"),
            P("sp", "tp"),
            P("sp", "tp"),
            P("sp", "tp"),
            P(),
            P(),
            P(),
            P(),
            P("sp", "tp"),
            P(),
            P(),
            P(),
            P("tp", "sp"),
            P("tp", "sp"),
        ),
        out_specs=P(("sp", "tp"), None),
        check_vma=False,
    )
```
